128 devices in a mesh: fs: 16 (over z, x), tp: 8 (over y, core).
Axes of the slice: x: 4, y: 4, z: 4, core: 2. Of those that a mesh axis runs over, the one named last changes fastest.
Arguments:
- query_rows: bfloat16 [32768, 2048], P('fs', 'tp'), may hold values from -16 to 16
- key_rows: bfloat16 [32768, 2048], P('fs', 'tp'), may hold values from -8 to 8
- value_rows: bfloat16 [32768, 2048], P('fs', 'tp'), may hold values from -6 to 6
- mix_lambda: float32 [16], P('tp'), may hold values from 0.3 to 0.8
- head_gain: float32 [128], replicated, may hold values from 0.1 to 1.9
- out_cotangent: bfloat16 [32768, 2048], P('fs'), may hold values from -0.049804688 to 0.049804688
- layer_input: bfloat16 [32768, 2048], P('fs'), may hold values from -6 to 6
- value_cotangent: bfloat16 [32768, 2048], P('fs', 'tp'), may hold values from -0.049804688 to 0.049804688
- out_weight: float32 [2048, 2048], P('tp', 'fs'), may hold values from -0.125 to 0.125
- value_weight: float32 [2048, 2048], P('fs', 'tp'), may hold values from -0.125 to 0.125
- out_basis: bfloat16 [2048, 256], replicated, may hold values from -0.125 to 0.125
- value_basis: bfloat16 [2048, 256], replicated, may hold values from -0.125 to 0.125
- out_first: float32 [256, 2048], P('fs', 'tp'), may hold values from -20 to 20
- out_second: float32 [256, 2048], P('fs', 'tp'), may hold values from 0.02 to 0.5
- value_first: float32 [256, 2048], P('fs', 'tp'), may hold values from -20 to 20
- value_second: float32 [256, 2048], P('fs', 'tp'), may hold values from 0.02 to 0.5
Outputs:
- out_step: float32 [2048, 2048], P('tp', 'fs')
- value_step: float32 [2048, 2048], P('fs', 'tp')
- new_out_weight: float32 [2048, 2048], P('tp', 'fs')
- new_value_weight: float32 [2048, 2048], P('fs', 'tp')
- out_copy: bfloat16 [2048, 2048], P('tp')
- value_copy: bfloat16 [2048, 2048], P(None, 'tp')
- new_out_first: float32 [256, 2048], P('fs', 'tp')
- new_out_second: float32 [256, 2048], P('fs', 'tp')
- new_value_first: float32 [256, 2048], P('fs', 'tp')
- new_value_second: float32 [256, 2048], P('fs', 'tp')
The draws below stay inside these ranges and needn't reach their ends.
All inputs are finite; a program needn't handle non-finite values.
Results may differ from the reference program's by a relative error of at most 0.001.
Values may be sent and summed in bfloat16 or wider, within the bound.
A program may use at most 128 MiB of HBM per device.

```python
import math
import jax
import jax.numpy as jnp
from jax import lax

D = 2048
H = 16
DH = 64
DV = 128
RANK = 256
LEN = 2048
TOKENS = 32768
V = 2048
QKW = 2048


def draw_query_rows(key, part):
    base_draw = jnp.clip(jax.random.normal(jax.random.fold_in(key, 1), (TOKENS // LEN, LEN, 2 * H, DH), jnp.float32) * 1.3, -5.2, 5.2)
    return jnp.clip(base_draw, -16.0, 16.0).reshape(TOKENS, QKW).astype(jnp.bfloat16)


def draw_key_rows(key, part):
    base_draw = jnp.clip(jax.random.normal(jax.random.fold_in(key, 2), (TOKENS // LEN, LEN, 2 * H, DH), jnp.float32) * 1.3, -5.2, 5.2)
    return jnp.clip(base_draw, -8.0, 8.0).reshape(TOKENS, QKW).astype(jnp.bfloat16)


def moment_draw(key, salt):
    row_rise = jnp.arange(RANK, dtype=jnp.float32)[:, None] / RANK
    col_rise = jnp.arange(V, dtype=jnp.float32)[None, :] / V
    jitter = jax.random.uniform(jax.random.fold_in(key, salt), (RANK, V), jnp.float32, -0.35, 0.35)
    scales = 0.3 * 10.0 ** (0.5 * (row_rise + col_rise)) * jnp.exp(jitter)
    values = jnp.clip(jax.random.normal(jax.random.fold_in(key, salt + 1), (RANK, V), jnp.float32), -4.0, 4.0)
    return jnp.clip(values * scales, -20.0, 20.0)


def draw_out_first(key, part):
    return moment_draw(key, 11)


def draw_value_first(key, part):
    return moment_draw(key, 21)


def shard_levels(key, shape, split, least, top_value):
    level = 1.0
    for axis_at, parts in split:
        heights = jax.random.uniform(jax.random.fold_in(jax.random.fold_in(key, 6), axis_at), (parts,), jnp.float32, least / len(split), top_value / len(split))
        level = level * jnp.repeat(jnp.exp(heights), shape[axis_at] // parts).reshape((-1,) + (1,) * (len(shape) - 1 - axis_at))
    return level


def scatter_about(key, shape, spread, reach, pieces=(), kind=jnp.bfloat16):
    drawn = jax.random.normal(key, shape, jnp.float32) * spread
    if len(pieces) > 0:
        drawn = shard_levels(key, shape, pieces, -0.22, 0.18) * drawn
    return jnp.clip(drawn, min=-reach, max=reach).astype(kind)


def setup_inputs(seed: int = 0) -> dict:
    key_list = jax.random.split(jax.random.key(seed), 17)
    return {
        "query_rows": draw_query_rows(jax.random.fold_in(key_list[16], 71), 0),
        "key_rows": draw_key_rows(jax.random.fold_in(key_list[16], 71), 0),
        "value_rows": scatter_about(key_list[2], (TOKENS, V), 1.0, 6.0, ((0, 16), (1, 8))),
        "mix_lambda": jnp.clip(0.3 + 0.5 * jax.random.uniform(key_list[3], (H,), jnp.float32) ** shard_levels(key_list[3], (H,), ((0, 8),), -0.2, 0.2), 0.3, 0.8),
        "head_gain": jnp.clip(1.0 + 0.18 * jax.random.normal(key_list[4], (DV,), jnp.float32), 0.1, 1.9),
        "out_cotangent": scatter_about(key_list[5], (TOKENS, D), 0.008, 0.049804688, ((0, 16),)),
        "layer_input": scatter_about(key_list[6], (TOKENS, D), 1.0, 6.0, ((0, 16),)),
        "value_cotangent": scatter_about(key_list[7], (TOKENS, V), 0.008, 0.049804688, ((0, 16), (1, 8))),
        "out_weight": scatter_about(key_list[8], (V, D), V ** -0.5, 0.125, ((0, 8), (1, 16)), jnp.float32),
        "value_weight": scatter_about(key_list[9], (D, V), D ** -0.5, 0.125, ((0, 16), (1, 8)), jnp.float32),
        "out_basis": scatter_about(key_list[10], (D, RANK), D ** -0.5, 0.125),
        "value_basis": scatter_about(key_list[11], (D, RANK), D ** -0.5, 0.125),
        "out_first": draw_out_first(jax.random.fold_in(key_list[16], 71), 0),
        "out_second": jnp.clip(jnp.exp(math.log(0.5) - 3.218876 * jax.random.uniform(key_list[13], (RANK, V), jnp.float32) ** shard_levels(key_list[13], (RANK, V), ((0, 16), (1, 8)), -0.2, 0.2)), 0.02, 0.5),
        "value_first": draw_value_first(jax.random.fold_in(key_list[16], 71), 0),
        "value_second": jnp.clip(jnp.exp(math.log(0.5) - 3.218876 * jax.random.uniform(key_list[15], (RANK, V), jnp.float32) ** shard_levels(key_list[15], (RANK, V), ((0, 16), (1, 8)), -0.2, 0.2)), 0.02, 0.5),
    }


EPSILON_NORM = 1e-05
EPSILON_ADAM = 1e-08
BETA_ONE = 0.9
BETA_TWO = 0.95
CLIP_RMS = 1.0
LEARN_RATE = 0.01

def moment_step(proj, first, second):
    new_first = BETA_ONE * first + (1.0 - BETA_ONE) * proj
    new_second = BETA_TWO * second + (1.0 - BETA_TWO) * proj * proj
    direction = new_first / (jnp.sqrt(new_second) + EPSILON_ADAM)
    return (new_first, new_second, direction)

def adapt(grad, basis, first, second):
    basis_wide = basis.astype(jnp.float32)
    proj = jnp.dot(basis_wide.T, grad, precision=lax.Precision.HIGHEST)
    new_first, new_second, direction = moment_step(proj, first, second)
    clip_factor = jnp.minimum(1.0, CLIP_RMS * math.sqrt(RANK * V) / jnp.sqrt(jnp.sum(direction * direction)))
    step_full = clip_factor * jnp.dot(basis_wide, direction, precision=lax.Precision.HIGHEST)
    return (step_full, new_first, new_second)

def reference(query_rows, key_rows, value_rows, mix_lambda, head_gain, out_cotangent, layer_input, value_cotangent, out_weight, value_weight, out_basis, value_basis, out_first, out_second, value_first, value_second):
    seq_count = TOKENS // LEN
    query_heads = query_rows.reshape(seq_count, LEN, H, 2, DH).transpose(0, 2, 3, 1, 4).reshape(seq_count * H, 2, LEN, DH)
    key_heads = key_rows.reshape(seq_count, LEN, H, 2, DH).transpose(0, 2, 3, 1, 4).reshape(seq_count * H, 2, LEN, DH)
    value_heads = value_rows.reshape(seq_count, LEN, H, DV).transpose(0, 2, 1, 3).reshape(seq_count * H, LEN, DV)
    lam_rows = jnp.tile(mix_lambda, seq_count)
    positions = jnp.arange(LEN)
    causal = positions[None, :] <= positions[:, None]

    def attend(operands):
        query_pair, key_pair, value_head, lam_value = operands
        scores = jnp.einsum('mqd,mkd->mqk', query_pair.astype(jnp.float32), key_pair.astype(jnp.float32)) * DH ** (-0.5)
        scores = jnp.where(causal[None], scores, -jnp.inf)
        row_peak = lax.optimization_barrier(jnp.max(scores, axis=-1, keepdims=True))
        exp_scores = jnp.exp(scores - row_peak)
        soft_maps = exp_scores / lax.optimization_barrier(jnp.sum(exp_scores, axis=-1, keepdims=True))
        mix_weights = (soft_maps[0] - lam_value * soft_maps[1]).astype(jnp.bfloat16)
        raw_out = jnp.dot(mix_weights, value_head, preferred_element_type=jnp.float32)
        normed = raw_out * lax.rsqrt(lax.optimization_barrier(jnp.mean(raw_out * raw_out, axis=-1, keepdims=True)) + EPSILON_NORM) * head_gain
        return normed.astype(jnp.bfloat16)
    head_blocks = lax.map(attend, (query_heads, key_heads, value_heads, lam_rows))
    head_out = head_blocks.reshape(seq_count, H, LEN, DV).transpose(0, 2, 1, 3).reshape(TOKENS, H * DV)
    out_grad = jnp.dot(out_cotangent.T, head_out, preferred_element_type=jnp.float32)
    value_grad = jnp.dot(layer_input.T, value_cotangent, preferred_element_type=jnp.float32)
    out_full, new_out_first, new_out_second = adapt(out_grad, out_basis, out_first, out_second)
    value_step, new_value_first, new_value_second = adapt(value_grad, value_basis, value_first, value_second)
    out_step = out_full.T
    new_out_weight = out_weight - LEARN_RATE * out_step
    new_value_weight = value_weight - LEARN_RATE * value_step
    return (out_step, value_step, new_out_weight, new_value_weight, new_out_weight.astype(jnp.bfloat16), new_value_weight.astype(jnp.bfloat16), new_out_first, new_out_second, new_value_first, new_value_second)
```

```python
import math

import jax
import jax.numpy as jnp
from jax import lax
from jax.experimental import pallas as pl
from jax.experimental.pallas import tpu as pltpu
from jax.sharding import Mesh
from jax.sharding import PartitionSpec as P

FS = ("fs_0", "fs_1")
TP = ("tp_0", "tp_1")

SEQ = 2048
WIDE = 2048
COLS = 256
RANK = 256
BLOCK = 256
FS_SIDE = 4
FS_COUNT = 16
SHARE = RANK // FS_COUNT
OWN = WIDE // FS_COUNT
DH = 64
DV = 128

EPSILON_NORM = 1e-05
EPSILON_ADAM = 1e-08
BETA_ONE = 0.9
BETA_TWO = 0.95
CLIP_RMS = 1.0
LEARN_RATE = 0.01
ENTRY_COUNT = RANK * WIDE
SCORE_SCALE = math.log2(math.e) * DH**-0.5

F32 = jnp.float32
BF16 = jnp.bfloat16
MESH = pl.DeviceIdType.MESH
NT = (((1,), (1,)), ((), ()))
NN = (((1,), (0,)), ((), ()))


def mul(a, b, dims=NN):
    return lax.dot_general(a, b, dims, preferred_element_type=F32)


def two_parts(value):
    high = value.astype(BF16)
    return high, (value - high.astype(F32)).astype(BF16)


def moment_step(proj, first, second):
    new_first = BETA_ONE * first + (1.0 - BETA_ONE) * proj
    new_second = BETA_TWO * second + (1.0 - BETA_TWO) * proj * proj
    direction = new_first / (jnp.sqrt(new_second) + EPSILON_ADAM)
    return (new_first, new_second, direction)


def column(row):
    return jnp.transpose(jnp.broadcast_to(row, (row.shape[1], row.shape[1])))


class Gather:
    def __init__(self, buf, send, recv, z, x):
        self.buf, self.send, self.recv = buf, send, recv
        self.pos = {"fs_0": z, "fs_1": x}
        self.rows = buf.shape[3]

    def at(self, half, where, part):
        rows = slice(None) if part is None else pl.ds(part * (self.rows // 2), self.rows // 2)
        first = where.get("fs_0", slice(None))
        second = where.get("fs_1", slice(None))
        return self.buf.at[first, second, half, rows]

    def copies(self, stage):
        phase, forward = divmod(stage, 2)
        out = []
        for half in range(2):
            order = FS if half == 0 else FS[::-1]
            axis = order[phase]
            other = order[1 - phase]
            for way in range(2):
                step = 1 if way == 0 else FS_SIDE - 1
                here = self.pos[axis]
                target = lax.rem(here + step, FS_SIDE)
                held = here if not forward else lax.rem(here + FS_SIDE - step, FS_SIDE)
                where = {axis: held}
                if phase == 0:
                    where[other] = self.pos[other]
                view = self.at(half, where, way if forward else None)
                index = stage * 4 + half * 2 + way
                out.append(
                    pltpu.make_async_remote_copy(
                        src_ref=view,
                        dst_ref=view,
                        send_sem=self.send.at[index],
                        recv_sem=self.recv.at[index],
                        device_id={axis: target},
                        device_id_type=MESH,
                    )
                )
        return out

    def start(self, stage):
        for copy in self.copies(stage):
            copy.start()

    def arrive(self, stage):
        for copy in self.copies(stage):
            copy.wait_recv()

    def finish(self):
        for stage in range(4):
            for copy in self.copies(stage):
                copy.wait_send()


def spread(z, x):
    for step in range(1, FS_COUNT):
        far_z = lax.rem(z + step // FS_SIDE, FS_SIDE)
        far_x = lax.rem(x + step % FS_SIDE, FS_SIDE)
        yield step, far_z, far_x


def shares_out(parts, landing, send, recv, z, x):
    return [
        pltpu.make_async_remote_copy(
            src_ref=parts.at[far_z * FS_SIDE + far_x],
            dst_ref=landing.at[step],
            send_sem=send.at[step],
            recv_sem=recv.at[step],
            device_id={"fs_0": far_z, "fs_1": far_x},
            device_id_type=MESH,
        )
        for step, far_z, far_x in spread(z, x)
    ]


def rows_out(rows, send, recv, z, x):
    mine = rows.at[z * FS_SIDE + x]
    return [
        pltpu.make_async_remote_copy(
            src_ref=mine,
            dst_ref=mine,
            send_sem=send.at[step],
            recv_sem=recv.at[step],
            device_id={"fs_0": far_z, "fs_1": far_x},
            device_id_type=MESH,
        )
        for step, far_z, far_x in spread(z, x)
    ]


def sums_out(sums, send, recv, y, c):
    return [
        pltpu.make_async_remote_copy(
            src_ref=sums.at[0],
            dst_ref=sums.at[step],
            send_sem=send.at[step],
            recv_sem=recv.at[step],
            device_id={
                "tp_0": lax.rem(y + step // 2, 4),
                "tp_1": lax.rem(c + step % 2, 2),
            },
            device_id_type=MESH,
        )
        for step in range(1, 8)
    ]


def start(copies):
    for copy in copies:
        copy.start()


def arrive(copies):
    for copy in copies:
        copy.wait_recv()


def finish(copies):
    for copy in copies:
        copy.wait_send()


def body(
    lam_ref,
    gain_ref,
    out_weight_ref,
    value_weight_ref,
    out_first_ref,
    out_second_ref,
    value_first_ref,
    value_second_ref,
    query_hbm,
    key_hbm,
    value_hbm,
    out_cot_hbm,
    layer_hbm,
    value_cot_hbm,
    out_basis_hbm,
    value_basis_hbm,
    out_step_ref,
    value_step_ref,
    new_out_weight_ref,
    new_value_weight_ref,
    out_copy_ref,
    value_copy_ref,
    new_out_first_ref,
    new_out_second_ref,
    new_value_first_ref,
    new_value_second_ref,
    query_ref,
    key_ref,
    value_ref,
    value_cot_ref,
    out_basis_ref,
    value_basis_ref,
    layer_ref,
    out_cot_ref,
    turned_ref,
    score_ref,
    weight_ref,
    head_ref,
    high_ref,
    low_ref,
    out_all_ref,
    value_all_ref,
    value_parts,
    value_landing,
    value_rows,
    value_sums,
    out_parts,
    out_landing,
    out_rows,
    out_sums,
    total_ref,
    local_sem,
    gather_out_send,
    gather_out_recv,
    gather_value_send,
    gather_value_recv,
    share_send,
    share_recv,
    row_send,
    row_recv,
    sum_send,
    sum_recv,
):
    z, x = lax.axis_index("fs_0"), lax.axis_index("fs_1")
    y, c = lax.axis_index("tp_0"), lax.axis_index("tp_1")
    me = z * FS_SIDE + x
    chunks = SEQ // BLOCK

    def span(n):
        return slice(n * BLOCK, (n + 1) * BLOCK)

    local = []

    def fetch(src, dst):
        copy = pltpu.make_async_copy(src, dst, local_sem.at[len(local)])
        local.append(copy)
        copy.start()
        return copy

    got_value_basis = fetch(value_basis_hbm, value_basis_ref)
    got_value_cot = fetch(value_cot_hbm, value_cot_ref)
    got_layer = [fetch(layer_hbm.at[span(n)], layer_ref.at[span(n)]) for n in range(chunks)]
    got_qkv = [
        fetch(query_hbm, query_ref),
        fetch(key_hbm, key_ref),
        fetch(value_hbm, value_ref),
    ]
    got_out_basis = fetch(out_basis_hbm, out_basis_ref)
    got_out_cot = [fetch(out_cot_hbm.at[span(n)], out_cot_ref.at[span(n)]) for n in range(chunks)]

    barrier = pltpu.get_barrier_semaphore()
    for _, far_z, far_x in spread(z, x):
        pl.semaphore_signal(
            barrier, inc=1, device_id={"fs_0": far_z, "fs_1": far_x}, device_id_type=MESH
        )
    for step in range(1, 8):
        pl.semaphore_signal(
            barrier,
            inc=1,
            device_id={"tp_0": lax.rem(y + step // 2, 4), "tp_1": lax.rem(c + step % 2, 2)},
            device_id_type=MESH,
        )
    out_all_ref[z, x, 0] = out_weight_ref[:128, :]
    out_all_ref[z, x, 1] = out_weight_ref[128:, :]
    pl.semaphore_wait(barrier, 22)

    gather_out = Gather(out_all_ref, gather_out_send, gather_out_recv, z, x)
    gather_value = Gather(value_all_ref, gather_value_send, gather_value_recv, z, x)
    value_shares = shares_out(value_parts, value_landing, share_send.at[0], share_recv.at[0], z, x)
    out_shares = shares_out(out_parts, out_landing, share_send.at[1], share_recv.at[1], z, x)
    value_row_copies = rows_out(value_rows, row_send.at[0], row_recv.at[0], z, x)
    out_row_copies = rows_out(out_rows, row_send.at[1], row_recv.at[1], z, x)
    value_sum_copies = sums_out(value_sums, sum_send.at[0], sum_recv.at[0], y, c)
    out_sum_copies = sums_out(out_sums, sum_send.at[1], sum_recv.at[1], y, c)

    gather_out.start(0)

    got_value_basis.wait()
    got_value_cot.wait()
    proj_t = None
    for n in range(chunks):
        got_layer[n].wait()
        wide = mul(layer_ref[span(n), :], value_basis_ref[...])
        high, low = two_parts(wide)
        turned = value_cot_ref[span(n), :].T
        part = mul(turned, high) + mul(turned, low)
        proj_t = part if proj_t is None else proj_t + part
    value_parts[...] = proj_t.T.reshape(FS_COUNT, SHARE, COLS)
    start(value_shares)
    gather_out.arrive(0)
    gather_out.start(1)

    for copy in got_qkv:
        copy.wait()
    got_out_basis.wait()
    for n in range(chunks):
        turned_ref[:, span(n)] = value_ref[span(n), :].T
    gain = column(gain_ref[...])
    gain = jnp.concatenate([gain, gain], axis=1)
    lane = lax.broadcasted_iota(jnp.int32, (BLOCK, 128), 1)
    causal = lax.broadcasted_iota(jnp.int32, (BLOCK, BLOCK), 0) <= lax.broadcasted_iota(
        jnp.int32, (BLOCK, BLOCK), 1
    )

    jobs = [(i, h) for i in range(chunks) for h in range(2)]

    def scores(n, peaks):
        i, h = jobs[n]
        both = []
        for m in range(2):
            scaled = query_ref[span(i), h * 128 : (h + 1) * 128].astype(F32) * SCORE_SCALE
            scaled = jnp.where((lane < DH) if m == 0 else (lane >= DH), scaled, 0.0)
            both.append(jnp.concatenate(two_parts(scaled), axis=1))
        best = [None, None]
        for j in range(i + 1):
            keys = key_ref[span(j), h * 128 : (h + 1) * 128]
            for m in range(2):
                s = mul(jnp.concatenate([keys, keys], axis=1), both[m], NT)
                if j == i:
                    s = jnp.where(causal, s, -jnp.inf)
                score_ref[n % 2, m, span(j), :] = s
                top = jnp.max(s.reshape(BLOCK // 8, 8, BLOCK), axis=0)
                best[m] = top if best[m] is None else jnp.maximum(best[m], top)
                yield
        peaks.extend(jnp.max(b, axis=0, keepdims=True) for b in best)

    def weigh(n, peaks):
        i, h = jobs[n]
        held = score_ref.at[n % 2]
        sums = [None, None]
        for j in range(i + 1):
            for m in range(2):
                e = jnp.exp2(held[m, span(j), :] - peaks[m])
                part = jnp.sum(e.reshape(BLOCK // 8, 8, BLOCK), axis=0)
                sums[m] = part if sums[m] is None else sums[m] + part
                held[m, span(j), :] = e
                yield
        sums = [jnp.sum(t, axis=0, keepdims=True) for t in sums]
        one, two = 1.0 / sums[0], lam_ref[h] / sums[1]
        for j in range(i + 1):
            mixed = held[0, span(j), :] * one - held[1, span(j), :] * two
            weight_ref[n % 2, span(j), :] = mixed.astype(BF16)
            yield
        depth = (i + 1) * BLOCK
        raw = mul(turned_ref[h * DV : (h + 1) * DV, :depth], weight_ref[n % 2, :depth, :])
        mean = jnp.mean(raw * raw, axis=0, keepdims=True)
        normed = raw * lax.rsqrt(mean + EPSILON_NORM) * gain
        head_ref[h * DV : (h + 1) * DV, span(i)] = normed.astype(BF16)

    def together(first, first_count, second, second_count):
        due = 0.0
        for _ in range(first_count):
            next(first, None)
            due += second_count / first_count
            while due >= 1.0:
                next(second, None)
                due -= 1.0
        for chain in (first, second):
            for _ in chain:
                pass

    def clip_of(sums):
        total = jnp.sum(sums[...], axis=0)[0:1, 0:1]
        return jnp.minimum(1.0, CLIP_RMS * math.sqrt(ENTRY_COUNT) / jnp.sqrt(total))

    def moments(parts, landing, first, second, new_first, new_second, rows):
        proj = parts[me]
        for step in range(1, FS_COUNT):
            proj = proj + landing[step]
        new_first[...], new_second[...], direction = moment_step(proj, first[...], second[...])
        rows[me] = direction

    def square_sum(rows, sums):
        every = rows[...].reshape(RANK, COLS)
        sums[0] = jnp.broadcast_to(jnp.sum(every * every, keepdims=True), (8, 128))

    def after(job):
        if job == 3:
            gather_out.arrive(1)
            gather_out.start(2)
        if job == 6:
            arrive(value_shares)
            moments(
                value_parts,
                value_landing,
                value_first_ref,
                value_second_ref,
                new_value_first_ref,
                new_value_second_ref,
                value_rows,
            )
            start(value_row_copies)
        if job == 9:
            arrive(value_row_copies)
            square_sum(value_rows, value_sums)
            start(value_sum_copies)
        if job == 10:
            gather_out.arrive(2)
            gather_out.start(3)
        if job == 11:
            arrive(value_sum_copies)
            high, low = two_parts(value_rows[...].reshape(RANK, COLS))
            own = value_basis_ref[pl.ds(pl.multiple_of(me * OWN, OWN), OWN), :]
            step = clip_of(value_sums) * (mul(own, high) + mul(own, low))
            value_step_ref[...] = step
            new = value_weight_ref[...] - LEARN_RATE * step
            new_value_weight_ref[...] = new
            value_all_ref[z, x] = new.astype(BF16).reshape(2, OWN // 2, COLS)
            gather_value.start(0)
        if job == 12:
            gather_value.arrive(0)
            gather_value.start(1)
        if job == 13:
            gather_value.arrive(1)
            gather_value.start(2)
        if job == 15:
            gather_value.arrive(2)
            gather_value.start(3)

    peaks = [[] for _ in jobs]
    for _ in scores(0, peaks[0]):
        pass
    for n, (i, h) in enumerate(jobs):
        if h == 0:
            got_out_cot[i].wait()
            wide = mul(out_cot_ref[span(i), :], out_basis_ref[...])
            high_ref[span(i), :], low_ref[span(i), :] = two_parts(wide)
        ahead, ahead_count = iter(()), 0
        if n + 1 < len(jobs):
            ahead, ahead_count = scores(n + 1, peaks[n + 1]), 2 * (jobs[n + 1][0] + 1) + 1
        together(weigh(n, peaks[n]), 3 * (i + 1) + 1, ahead, ahead_count)
        after(n)

    proj_t = mul(head_ref[...], high_ref[...]) + mul(head_ref[...], low_ref[...])
    out_parts[...] = proj_t.T.reshape(FS_COUNT, SHARE, COLS)
    start(out_shares)
    arrive(out_shares)
    moments(
        out_parts,
        out_landing,
        out_first_ref,
        out_second_ref,
        new_out_first_ref,
        new_out_second_ref,
        out_rows,
    )
    start(out_row_copies)
    gather_out.arrive(3)
    gather_value.arrive(3)
    for at in range(FS_COUNT):
        value_copy_ref[at * OWN : (at + 1) * OWN, :] = value_all_ref[
            at // FS_SIDE, at % FS_SIDE
        ].reshape(OWN, COLS)
    arrive(out_row_copies)
    square_sum(out_rows, out_sums)
    start(out_sum_copies)
    high, low = two_parts(out_rows[...].reshape(RANK, COLS).T)
    for at in range(FS_COUNT):
        basis = out_basis_ref[at * OWN : (at + 1) * OWN, :]
        total_ref[at] = mul(high, basis, NT) + mul(low, basis, NT)
    arrive(out_sum_copies)
    clip = clip_of(out_sums)
    step = clip * total_ref[me]
    out_step_ref[...] = step
    new_out_weight_ref[...] = out_weight_ref[...] - LEARN_RATE * step
    for at in range(FS_COUNT):
        old = out_all_ref[at // FS_SIDE, at % FS_SIDE].reshape(COLS, OWN)
        new = old - LEARN_RATE * (clip * total_ref[at])
        out_copy_ref[:, at * OWN : (at + 1) * OWN] = new.astype(BF16)

    gather_out.finish()
    gather_value.finish()
    for copies in (
        value_shares,
        out_shares,
        value_row_copies,
        out_row_copies,
        value_sum_copies,
        out_sum_copies,
    ):
        finish(copies)


def step(
    query_rows,
    key_rows,
    value_rows,
    mix_lambda,
    head_gain,
    out_cotangent,
    layer_input,
    value_cotangent,
    out_weight,
    value_weight,
    out_basis,
    value_basis,
    out_first,
    out_second,
    value_first,
    value_second,
):
    vmem = pl.BlockSpec(memory_space=pltpu.VMEM)
    smem = pl.BlockSpec(memory_space=pltpu.SMEM)
    anywhere = pl.BlockSpec(memory_space=pl.ANY)
    dma = pltpu.SemaphoreType.DMA
    shape = jax.ShapeDtypeStruct
    return pl.pallas_call(
        body,
        out_shape=(
            shape((COLS, OWN), F32),
            shape((OWN, COLS), F32),
            shape((COLS, OWN), F32),
            shape((OWN, COLS), F32),
            shape((COLS, WIDE), BF16),
            shape((WIDE, COLS), BF16),
            shape((SHARE, COLS), F32),
            shape((SHARE, COLS), F32),
            shape((SHARE, COLS), F32),
            shape((SHARE, COLS), F32),
        ),
        in_specs=[smem] + [vmem] * 7 + [anywhere] * 8,
        out_specs=(vmem,) * 10,
        scratch_shapes=[
            pltpu.VMEM((SEQ, COLS), BF16),
            pltpu.VMEM((SEQ, COLS), BF16),
            pltpu.VMEM((SEQ, COLS), BF16),
            pltpu.VMEM((SEQ, COLS), BF16),
            pltpu.VMEM((WIDE, RANK), BF16),
            pltpu.VMEM((WIDE, RANK), BF16),
            pltpu.VMEM((SEQ, WIDE), BF16),
            pltpu.VMEM((SEQ, WIDE), BF16),
            pltpu.VMEM((COLS, SEQ), BF16),
            pltpu.VMEM((2, 2, SEQ, BLOCK), F32),
            pltpu.VMEM((2, SEQ, BLOCK), BF16),
            pltpu.VMEM((COLS, SEQ), BF16),
            pltpu.VMEM((SEQ, RANK), BF16),
            pltpu.VMEM((SEQ, RANK), BF16),
            pltpu.VMEM((FS_SIDE, FS_SIDE, 2, COLS // 2, OWN), F32),
            pltpu.VMEM((FS_SIDE, FS_SIDE, 2, OWN // 2, COLS), BF16),
            pltpu.VMEM((FS_COUNT, SHARE, COLS), F32),
            pltpu.VMEM((FS_COUNT, SHARE, COLS), F32),
            pltpu.VMEM((FS_COUNT, SHARE, COLS), F32),
            pltpu.VMEM((8, 8, 128), F32),
            pltpu.VMEM((FS_COUNT, SHARE, COLS), F32),
            pltpu.VMEM((FS_COUNT, SHARE, COLS), F32),
            pltpu.VMEM((FS_COUNT, SHARE, COLS), F32),
            pltpu.VMEM((8, 8, 128), F32),
            pltpu.VMEM((FS_COUNT, COLS, OWN), F32),
            dma((32,)),
            dma((16,)),
            dma((16,)),
            dma((16,)),
            dma((16,)),
            dma((2, 16)),
            dma((2, 16)),
            dma((2, 16)),
            dma((2, 16)),
            dma((2, 8)),
            dma((2, 8)),
        ],
        compiler_params=pltpu.CompilerParams(
            collective_id=0, has_side_effects=True, vmem_limit_bytes=62 * 2**20
        ),
    )(
        mix_lambda,
        head_gain.reshape(1, DV),
        out_weight,
        value_weight,
        out_first,
        out_second,
        value_first,
        value_second,
        query_rows,
        key_rows,
        value_rows,
        out_cotangent,
        layer_input,
        value_cotangent,
        out_basis,
        value_basis,
    )


def solution(mesh):
    torus = Mesh(mesh.devices.reshape(4, 4, 4, 2), FS + TP)
    sliced = P(FS, TP)
    return jax.shard_map(
        step,
        mesh=torus,
        in_specs=(
            sliced,
            sliced,
            sliced,
            P(TP),
            P(),
            P(FS, None),
            P(FS, None),
            sliced,
            P(TP, FS),
            sliced,
            P(),
            P(),
            sliced,
            sliced,
            sliced,
            sliced,
        ),
        out_specs=(
            P(TP, FS),
            sliced,
            P(TP, FS),
            sliced,
            P(TP, None),
            P(None, TP),
            sliced,
            sliced,
            sliced,
            sliced,
        ),
        check_vma=False,
    )
```

```python
import math

import jax
import jax.numpy as jnp
from jax import lax
from jax.experimental import pallas as pl
from jax.experimental.pallas import tpu as pltpu
from jax.sharding import Mesh
from jax.sharding import PartitionSpec as P

FS = ("fs_0", "fs_1")
TP = ("tp_0", "tp_1")

SEQ = 2048
WIDE = 2048
COLS = 256
RANK = 256
BLOCK = 256
FS_SIDE = 4
FS_COUNT = 16
SHARE = RANK // FS_COUNT
OWN = WIDE // FS_COUNT
DH = 64
DV = 128

EPSILON_NORM = 1e-05
EPSILON_ADAM = 1e-08
BETA_ONE = 0.9
BETA_TWO = 0.95
CLIP_RMS = 1.0
LEARN_RATE = 0.01
ENTRY_COUNT = RANK * WIDE
SCORE_SCALE = math.log2(math.e) * DH**-0.5

F32 = jnp.float32
BF16 = jnp.bfloat16
MESH = pl.DeviceIdType.MESH
NT = (((1,), (1,)), ((), ()))
NN = (((1,), (0,)), ((), ()))


def mul(a, b, dims=NN):
    return lax.dot_general(a, b, dims, preferred_element_type=F32)


def two_parts(value):
    high = value.astype(BF16)
    return high, (value - high.astype(F32)).astype(BF16)


def moment_step(proj, first, second):
    new_first = BETA_ONE * first + (1.0 - BETA_ONE) * proj
    new_second = BETA_TWO * second + (1.0 - BETA_TWO) * proj * proj
    direction = new_first / (jnp.sqrt(new_second) + EPSILON_ADAM)
    return (new_first, new_second, direction)


def column(row):
    return jnp.transpose(jnp.broadcast_to(row, (row.shape[1], row.shape[1])))


class Gather:
    def __init__(self, buf, send, recv, z, x):
        self.buf, self.send, self.recv = buf, send, recv
        self.pos = {"fs_0": z, "fs_1": x}
        self.rows = buf.shape[3]

    def at(self, half, where, part):
        rows = slice(None) if part is None else pl.ds(part * (self.rows // 2), self.rows // 2)
        first = where.get("fs_0", slice(None))
        second = where.get("fs_1", slice(None))
        return self.buf.at[first, second, half, rows]

    def copies(self, stage):
        phase, forward = divmod(stage, 2)
        out = []
        for half in range(2):
            order = FS if half == 0 else FS[::-1]
            axis = order[phase]
            other = order[1 - phase]
            for way in range(2):
                step = 1 if way == 0 else FS_SIDE - 1
                here = self.pos[axis]
                target = lax.rem(here + step, FS_SIDE)
                held = here if not forward else lax.rem(here + FS_SIDE - step, FS_SIDE)
                where = {axis: held}
                if phase == 0:
                    where[other] = self.pos[other]
                view = self.at(half, where, way if forward else None)
                index = stage * 4 + half * 2 + way
                out.append(
                    pltpu.make_async_remote_copy(
                        src_ref=view,
                        dst_ref=view,
                        send_sem=self.send.at[index],
                        recv_sem=self.recv.at[index],
                        device_id={axis: target},
                        device_id_type=MESH,
                    )
                )
        return out

    def start(self, stage):
        for copy in self.copies(stage):
            copy.start()

    def arrive(self, stage):
        for copy in self.copies(stage):
            copy.wait_recv()

    def finish(self):
        for stage in range(4):
            for copy in self.copies(stage):
                copy.wait_send()


def spread(z, x):
    for step in range(1, FS_COUNT):
        far_z = lax.rem(z + step // FS_SIDE, FS_SIDE)
        far_x = lax.rem(x + step % FS_SIDE, FS_SIDE)
        yield step, far_z, far_x


def shares_out(parts, landing, send, recv, z, x):
    return [
        pltpu.make_async_remote_copy(
            src_ref=parts.at[far_z * FS_SIDE + far_x],
            dst_ref=landing.at[step],
            send_sem=send.at[step],
            recv_sem=recv.at[step],
            device_id={"fs_0": far_z, "fs_1": far_x},
            device_id_type=MESH,
        )
        for step, far_z, far_x in spread(z, x)
    ]


def rows_out(rows, send, recv, z, x):
    mine = rows.at[z * FS_SIDE + x]
    return [
        pltpu.make_async_remote_copy(
            src_ref=mine,
            dst_ref=mine,
            send_sem=send.at[step],
            recv_sem=recv.at[step],
            device_id={"fs_0": far_z, "fs_1": far_x},
            device_id_type=MESH,
        )
        for step, far_z, far_x in spread(z, x)
    ]


def sums_out(sums, send, recv, y, c):
    return [
        pltpu.make_async_remote_copy(
            src_ref=sums.at[0],
            dst_ref=sums.at[step],
            send_sem=send.at[step],
            recv_sem=recv.at[step],
            device_id={
                "tp_0": lax.rem(y + step // 2, 4),
                "tp_1": lax.rem(c + step % 2, 2),
            },
            device_id_type=MESH,
        )
        for step in range(1, 8)
    ]


def totals_out(totals, send, recv, z, x):
    return [
        pltpu.make_async_remote_copy(
            src_ref=totals.at[0],
            dst_ref=totals.at[step],
            send_sem=send.at[step],
            recv_sem=recv.at[step],
            device_id={"fs_0": far_z, "fs_1": far_x},
            device_id_type=MESH,
        )
        for step, far_z, far_x in spread(z, x)
    ]


def start(copies):
    for copy in copies:
        copy.start()


def arrive(copies):
    for copy in copies:
        copy.wait_recv()


def finish(copies):
    for copy in copies:
        copy.wait_send()


def body(
    lam_ref,
    gain_ref,
    out_weight_ref,
    value_weight_ref,
    out_first_ref,
    out_second_ref,
    value_first_ref,
    value_second_ref,
    query_hbm,
    key_hbm,
    value_hbm,
    out_cot_hbm,
    layer_hbm,
    value_cot_hbm,
    out_basis_hbm,
    value_basis_hbm,
    out_step_ref,
    value_step_ref,
    new_out_weight_ref,
    new_value_weight_ref,
    out_copy_ref,
    value_copy_ref,
    new_out_first_ref,
    new_out_second_ref,
    new_value_first_ref,
    new_value_second_ref,
    query_ref,
    key_ref,
    value_ref,
    value_cot_ref,
    out_basis_ref,
    value_basis_ref,
    layer_ref,
    out_cot_ref,
    turned_ref,
    score_ref,
    weight_ref,
    head_ref,
    high_ref,
    low_ref,
    out_all_ref,
    value_parts,
    value_landing,
    value_rows,
    value_sums,
    value_totals,
    out_parts,
    out_landing,
    out_rows,
    out_sums,
    out_totals,
    out_full_ref,
    proj_ref,
    local_sem,
    gather_out_send,
    gather_out_recv,
    gather_value_send,
    gather_value_recv,
    share_send,
    share_recv,
    row_send,
    row_recv,
    sum_send,
    sum_recv,
    total_send,
    total_recv,
):
    z, x = lax.axis_index("fs_0"), lax.axis_index("fs_1")
    y, c = lax.axis_index("tp_0"), lax.axis_index("tp_1")
    me = z * FS_SIDE + x
    chunks = SEQ // BLOCK

    def span(n):
        return slice(n * BLOCK, (n + 1) * BLOCK)

    local = []

    def fetch(src, dst):
        copy = pltpu.make_async_copy(src, dst, local_sem.at[len(local)])
        local.append(copy)
        copy.start()
        return copy

    def part(n):
        return slice(n * 2 * BLOCK, (n + 1) * 2 * BLOCK)

    got_value_basis = fetch(value_basis_hbm, value_basis_ref)
    got_layer = [fetch(layer_hbm.at[part(0)], layer_ref.at[part(0)])]
    got_value_cot = fetch(value_cot_hbm, value_cot_ref)
    for n in range(1, chunks // 2):
        got_layer.append(fetch(layer_hbm.at[part(n)], layer_ref.at[part(n)]))
    got_qkv = [
        fetch(query_hbm, query_ref),
        fetch(key_hbm, key_ref),
        fetch(value_hbm, value_ref),
    ]
    got_out_basis = fetch(out_basis_hbm, out_basis_ref)
    barrier = pltpu.get_barrier_semaphore()
    for _, far_z, far_x in spread(z, x):
        pl.semaphore_signal(
            barrier, inc=1, device_id={"fs_0": far_z, "fs_1": far_x}, device_id_type=MESH
        )
    for step in range(1, 8):
        pl.semaphore_signal(
            barrier,
            inc=1,
            device_id={"tp_0": lax.rem(y + step // 2, 4), "tp_1": lax.rem(c + step % 2, 2)},
            device_id_type=MESH,
        )
    out_all_ref[z, x, 0] = out_weight_ref[:128, :]
    out_all_ref[z, x, 1] = out_weight_ref[128:, :]

    gather_out = Gather(out_all_ref, gather_out_send, gather_out_recv, z, x)
    gather_value = Gather(value_copy_ref, gather_value_send, gather_value_recv, z, x)
    gathers = (gather_out, gather_value)
    value_shares = shares_out(value_parts, value_landing, share_send.at[0], share_recv.at[0], z, x)
    out_shares = shares_out(out_parts, out_landing, share_send.at[1], share_recv.at[1], z, x)
    value_row_copies = rows_out(value_rows, row_send.at[0], row_recv.at[0], z, x)
    out_row_copies = rows_out(out_rows, row_send.at[1], row_recv.at[1], z, x)
    value_sum_copies = sums_out(value_sums, sum_send.at[0], sum_recv.at[0], y, c)
    out_sum_copies = sums_out(out_sums, sum_send.at[1], sum_recv.at[1], y, c)
    value_total_copies = totals_out(value_totals, total_send.at[0], total_recv.at[0], z, x)
    out_total_copies = totals_out(out_totals, total_send.at[1], total_recv.at[1], z, x)

    got_value_basis.wait()
    for n in range(chunks // 2):
        got_layer[n].wait()
        if n == 1:
            got_value_cot.wait()
            pl.semaphore_wait(barrier, 22)
            gather_out.start(0)
        if n == 3:
            got_out_cot = [
                fetch(out_cot_hbm.at[span(t)], out_cot_ref.at[span(t)]) for t in range(chunks)
            ]
        wide = mul(layer_ref[part(n), :], value_basis_ref[...])
        high_ref[part(n), :], low_ref[part(n), :] = two_parts(wide)
        if n == 1:
            for t in range(chunks):
                head_ref[:, span(t)] = value_cot_ref[span(t), :].T
    proj_t = mul(head_ref[...], high_ref[...]) + mul(head_ref[...], low_ref[...])
    value_parts[...] = proj_t.T.reshape(FS_COUNT, SHARE, COLS)
    gather_out.arrive(0)
    gather_out.start(1)
    start(value_shares)

    for copy in got_qkv:
        copy.wait()
    got_out_basis.wait()
    turned_ref[:, span(0)] = value_ref[span(0), :].T
    gain = column(gain_ref[...])
    gain = jnp.concatenate([gain, gain], axis=1)
    lane = lax.broadcasted_iota(jnp.int32, (BLOCK, 128), 1)
    causal = lax.broadcasted_iota(jnp.int32, (BLOCK, BLOCK), 0) <= lax.broadcasted_iota(
        jnp.int32, (BLOCK, BLOCK), 1
    )

    jobs = [(i, h) for i in range(chunks) for h in range(2)]

    def scores(n, peaks):
        i, h = jobs[n]
        both = []
        for m in range(2):
            scaled = query_ref[span(i), h * 128 : (h + 1) * 128].astype(F32) * SCORE_SCALE
            scaled = jnp.where((lane < DH) if m == 0 else (lane >= DH), scaled, 0.0)
            both.append(jnp.concatenate(two_parts(scaled), axis=1))
        best = [None, None]
        for j in range(i + 1):
            keys = key_ref[span(j), h * 128 : (h + 1) * 128]
            for m in range(2):
                s = mul(jnp.concatenate([keys, keys], axis=1), both[m], NT)
                if j == i:
                    s = jnp.where(causal, s, -jnp.inf)
                score_ref[n % 2, m, span(j), :] = s
                top = jnp.max(s.reshape(BLOCK // 8, 8, BLOCK), axis=0)
                best[m] = top if best[m] is None else jnp.maximum(best[m], top)
                yield
        peaks.extend(jnp.max(b, axis=0, keepdims=True) for b in best)

    def weigh(n, peaks):
        i, h = jobs[n]
        held = score_ref.at[n % 2]
        sums = [None, None]
        for j in range(i + 1):
            for m in range(2):
                e = jnp.exp2(held[m, span(j), :] - peaks[m])
                part = jnp.sum(e.reshape(BLOCK // 8, 8, BLOCK), axis=0)
                sums[m] = part if sums[m] is None else sums[m] + part
                held[m, span(j), :] = e
                yield
        sums = [jnp.sum(t, axis=0, keepdims=True) for t in sums]
        one, two = 1.0 / sums[0], lam_ref[h] / sums[1]
        for j in range(i + 1):
            mixed = held[0, span(j), :] * one - held[1, span(j), :] * two
            weight_ref[n % 2, span(j), :] = mixed.astype(BF16)
            yield
        depth = (i + 1) * BLOCK
        raw = mul(turned_ref[h * DV : (h + 1) * DV, :depth], weight_ref[n % 2, :depth, :])
        mean = jnp.mean(raw * raw, axis=0, keepdims=True)
        normed = raw * lax.rsqrt(mean + EPSILON_NORM) * gain
        head_ref[h * DV : (h + 1) * DV, span(i)] = normed.astype(BF16)

    def together(first, first_count, second, second_count):
        due = 0.0
        for _ in range(first_count):
            next(first, None)
            due += second_count / first_count
            while due >= 1.0:
                next(second, None)
                due -= 1.0
        for chain in (first, second):
            for _ in chain:
                pass

    def clip_of(totals):
        total = jnp.sum(jnp.sum(totals[...], axis=0), keepdims=True)
        return jnp.minimum(1.0, CLIP_RMS * math.sqrt(ENTRY_COUNT) / jnp.sqrt(total))

    def moments(parts, landing, first, second, new_first, new_second, rows, sums):
        proj = parts[me]
        for step in range(1, FS_COUNT):
            proj = proj + landing[step]
        new_first[...], new_second[...], direction = moment_step(proj, first[...], second[...])
        rows[me] = direction
        square = direction * direction
        sums[0] = square[:8, :128] + square[8:, :128] + square[:8, 128:] + square[8:, 128:]

    def gather_next(gather, stage):
        gather.arrive(stage)
        if stage < 3:
            gather.start(stage + 1)

    def after(n):
        if n == 4:
            gather_next(gather_out, 1)
        if n == 7:
            arrive(value_shares)
            moments(
                value_parts,
                value_landing,
                value_first_ref,
                value_second_ref,
                new_value_first_ref,
                new_value_second_ref,
                value_rows,
                value_sums,
            )
            start(value_sum_copies)
            start(value_row_copies)
        if n == 10:
            arrive(value_sum_copies)
            value_totals[0] = jnp.sum(value_sums[...], axis=0)
            start(value_total_copies)
        if n == 12:
            gather_next(gather_out, 2)
        if n == 14:
            arrive(value_row_copies)
            arrive(value_total_copies)
            high, low = two_parts(value_rows[...].reshape(RANK, COLS))
            own = value_basis_ref[pl.ds(pl.multiple_of(me * OWN, OWN), OWN), :]
            step = clip_of(value_totals) * (mul(own, high) + mul(own, low))
            value_step_ref[...] = step
            new = value_weight_ref[...] - LEARN_RATE * step
            new_value_weight_ref[...] = new
            value_copy_ref[z, x] = new.astype(BF16).reshape(2, OWN // 2, COLS)
            gather_value.start(0)

    def widen(n):
        wide = mul(out_cot_ref[span(n), :], out_basis_ref[...])
        high_ref[span(n), :], low_ref[span(n), :] = two_parts(wide)

    def project(low, high):
        rows = slice(low * BLOCK, high * BLOCK)
        return mul(head_ref[:, rows], high_ref[rows, :]) + mul(head_ref[:, rows], low_ref[rows, :])

    wide_at = {3: 0, 5: 1, 7: 2, 8: 3, 9: 4, 10: 5, 11: 6, 12: 7}

    def extra(n):
        i, h = jobs[n]
        if n in wide_at:
            widen(wide_at[n])
        if n == 13:
            proj_ref[...] = project(0, 5)
        if n == 15:
            proj_ref[...] += project(5, 7)
        if h == 1 and i + 1 < chunks:
            turned_ref[:, span(i + 1)] = value_ref[span(i + 1), :].T

    peaks = [[] for _ in jobs]
    for _ in scores(0, peaks[0]):
        pass
    for n, (i, h) in enumerate(jobs):
        if n in wide_at:
            got_out_cot[wide_at[n]].wait()
        extra(n)
        ahead, ahead_count = iter(()), 0
        if n + 1 < len(jobs):
            ahead, ahead_count = scores(n + 1, peaks[n + 1]), 2 * (jobs[n + 1][0] + 1) + 1
        together(weigh(n, peaks[n]), 3 * (i + 1) + 1, ahead, ahead_count)
        after(n)

    proj_t = proj_ref[...] + project(7, 8)
    out_parts[...] = proj_t.T.reshape(FS_COUNT, SHARE, COLS)
    start(out_shares)
    gather_next(gather_value, 0)
    gather_next(gather_value, 1)
    arrive(out_shares)
    moments(
        out_parts,
        out_landing,
        out_first_ref,
        out_second_ref,
        new_out_first_ref,
        new_out_second_ref,
        out_rows,
        out_sums,
    )
    start(out_sum_copies)
    start(out_row_copies)
    arrive(out_sum_copies)
    out_totals[0] = jnp.sum(out_sums[...], axis=0)
    start(out_total_copies)
    gather_next(gather_value, 2)
    gather_next(gather_out, 3)
    arrive(out_row_copies)
    both = jnp.concatenate(two_parts(out_rows[...].reshape(RANK, COLS).T), axis=0)
    for n in range(chunks):
        full = mul(both, out_basis_ref[span(n), :], NT)
        out_full_ref[:, span(n)] = full[:COLS] + full[COLS:]
    arrive(out_total_copies)
    clip = clip_of(out_totals)
    own = pl.ds(pl.multiple_of(me * OWN, OWN), OWN)
    step = clip * out_full_ref[:, own]
    out_step_ref[...] = step
    new_out_weight_ref[...] = out_weight_ref[...] - LEARN_RATE * step
    for at in range(FS_COUNT):
        old = out_all_ref[at // FS_SIDE, at % FS_SIDE].reshape(COLS, OWN)
        cols = slice(at * OWN, (at + 1) * OWN)
        new = old - LEARN_RATE * (clip * out_full_ref[:, cols])
        out_copy_ref[:, cols] = new.astype(BF16)

    gather_next(gather_value, 3)
    for gather in gathers:
        gather.finish()
    for copies in (
        value_shares,
        out_shares,
        value_row_copies,
        out_row_copies,
        value_sum_copies,
        out_sum_copies,
        value_total_copies,
        out_total_copies,
    ):
        finish(copies)


def hand_over(*refs):
    count = len(refs) // 3
    given, taken, held = refs[:count], refs[count : 2 * count], refs[2 * count : 3 * count]
    sems = refs[3 * count]
    loads = [pltpu.make_async_copy(a, b, sems.at[0, n]) for n, (a, b) in enumerate(zip(given, held))]
    stores = [pltpu.make_async_copy(a, b, sems.at[1, n]) for n, (a, b) in enumerate(zip(held, taken))]
    start(loads)
    for load, store in zip(loads, stores):
        load.wait()
        store.start()
    for store in stores:
        store.wait()


def results(arrays):
    anywhere = pl.BlockSpec(memory_space=pl.ANY)
    return pl.pallas_call(
        hand_over,
        out_shape=tuple(jax.ShapeDtypeStruct(a.shape, a.dtype) for a in arrays),
        in_specs=[anywhere] * len(arrays),
        out_specs=(anywhere,) * len(arrays),
        scratch_shapes=[pltpu.VMEM(a.shape, a.dtype) for a in arrays]
        + [pltpu.SemaphoreType.DMA((2, len(arrays)))],
    )(*arrays)


def step(
    query_rows,
    key_rows,
    value_rows,
    mix_lambda,
    head_gain,
    out_cotangent,
    layer_input,
    value_cotangent,
    out_weight,
    value_weight,
    out_basis,
    value_basis,
    out_first,
    out_second,
    value_first,
    value_second,
):
    vmem = pl.BlockSpec(memory_space=pltpu.VMEM)
    smem = pl.BlockSpec(memory_space=pltpu.SMEM)
    anywhere = pl.BlockSpec(memory_space=pl.ANY)
    dma = pltpu.SemaphoreType.DMA
    shape = jax.ShapeDtypeStruct
    arrays = pl.pallas_call(
        body,
        out_shape=(
            shape((COLS, OWN), F32),
            shape((OWN, COLS), F32),
            shape((COLS, OWN), F32),
            shape((OWN, COLS), F32),
            shape((COLS, WIDE), BF16),
            shape((FS_SIDE, FS_SIDE, 2, OWN // 2, COLS), BF16),
            shape((SHARE, COLS), F32),
            shape((SHARE, COLS), F32),
            shape((SHARE, COLS), F32),
            shape((SHARE, COLS), F32),
        ),
        in_specs=[smem] + [vmem] * 7 + [anywhere] * 8,
        out_specs=(vmem,) * 10,
        scratch_shapes=[
            pltpu.VMEM((SEQ, COLS), BF16),
            pltpu.VMEM((SEQ, COLS), BF16),
            pltpu.VMEM((SEQ, COLS), BF16),
            pltpu.VMEM((SEQ, COLS), BF16),
            pltpu.VMEM((WIDE, RANK), BF16),
            pltpu.VMEM((WIDE, RANK), BF16),
            pltpu.VMEM((SEQ, WIDE), BF16),
            pltpu.VMEM((SEQ, WIDE), BF16),
            pltpu.VMEM((COLS, SEQ), BF16),
            pltpu.VMEM((2, 2, SEQ, BLOCK), F32),
            pltpu.VMEM((2, SEQ, BLOCK), BF16),
            pltpu.VMEM((COLS, SEQ), BF16),
            pltpu.VMEM((SEQ, RANK), BF16),
            pltpu.VMEM((SEQ, RANK), BF16),
            pltpu.VMEM((FS_SIDE, FS_SIDE, 2, COLS // 2, OWN), F32),
            pltpu.VMEM((FS_COUNT, SHARE, COLS), F32),
            pltpu.VMEM((FS_COUNT, SHARE, COLS), F32),
            pltpu.VMEM((FS_COUNT, SHARE, COLS), F32),
            pltpu.VMEM((8, 8, 128), F32),
            pltpu.VMEM((FS_COUNT, 8, 128), F32),
            pltpu.VMEM((FS_COUNT, SHARE, COLS), F32),
            pltpu.VMEM((FS_COUNT, SHARE, COLS), F32),
            pltpu.VMEM((FS_COUNT, SHARE, COLS), F32),
            pltpu.VMEM((8, 8, 128), F32),
            pltpu.VMEM((FS_COUNT, 8, 128), F32),
            pltpu.VMEM((COLS, WIDE), F32),
            pltpu.VMEM((COLS, RANK), F32),
            dma((32,)),
            dma((16,)),
            dma((16,)),
            dma((16,)),
            dma((16,)),
            dma((2, 16)),
            dma((2, 16)),
            dma((2, 16)),
            dma((2, 16)),
            dma((2, 8)),
            dma((2, 8)),
            dma((2, 16)),
            dma((2, 16)),
        ],
        compiler_params=pltpu.CompilerParams(
            collective_id=0, has_side_effects=True, vmem_limit_bytes=62 * 2**20
        ),
    )(
        mix_lambda,
        head_gain.reshape(1, DV),
        out_weight,
        value_weight,
        out_first,
        out_second,
        value_first,
        value_second,
        query_rows,
        key_rows,
        value_rows,
        out_cotangent,
        layer_input,
        value_cotangent,
        out_basis,
        value_basis,
    )
    copy = arrays[5].reshape(WIDE, COLS)
    return results((*arrays[:5], copy, *arrays[6:]))


def solution(mesh):
    torus = Mesh(mesh.devices.reshape(4, 4, 4, 2), FS + TP)
    sliced = P(FS, TP)
    return jax.shard_map(
        step,
        mesh=torus,
        in_specs=(
            sliced,
            sliced,
            sliced,
            P(TP),
            P(),
            P(FS, None),
            P(FS, None),
            sliced,
            P(TP, FS),
            sliced,
            P(),
            P(),
            sliced,
            sliced,
            sliced,
            sliced,
        ),
        out_specs=(
            P(TP, FS),
            sliced,
            P(TP, FS),
            sliced,
            P(TP, None),
            P(None, TP),
            sliced,
            sliced,
            sliced,
            sliced,
        ),
        check_vma=False,
    )
```

```python
import math

import jax
import jax.numpy as jnp
from jax import lax
from jax.experimental import pallas as pl
from jax.experimental.pallas import tpu as pltpu
from jax.sharding import Mesh
from jax.sharding import PartitionSpec as P

FS = ("fs_0", "fs_1")
TP = ("tp_0", "tp_1")

SEQ = 2048
WIDE = 2048
COLS = 256
RANK = 256
BLOCK = 256
FS_SIDE = 4
FS_COUNT = 16
SHARE = RANK // FS_COUNT
OWN = WIDE // FS_COUNT
DH = 64
DV = 128

EPSILON_NORM = 1e-05
EPSILON_ADAM = 1e-08
BETA_ONE = 0.9
BETA_TWO = 0.95
CLIP_RMS = 1.0
LEARN_RATE = 0.01
ENTRY_COUNT = RANK * WIDE
SCORE_SCALE = math.log2(math.e) * DH**-0.5

F32 = jnp.float32
BF16 = jnp.bfloat16
MESH = pl.DeviceIdType.MESH
NT = (((1,), (1,)), ((), ()))
NN = (((1,), (0,)), ((), ()))


def mul(a, b, dims=NN):
    return lax.dot_general(a, b, dims, preferred_element_type=F32)


def two_parts(value):
    high = value.astype(BF16)
    return high, (value - high.astype(F32)).astype(BF16)


def moment_step(proj, first, second):
    new_first = BETA_ONE * first + (1.0 - BETA_ONE) * proj
    new_second = BETA_TWO * second + (1.0 - BETA_TWO) * proj * proj
    direction = new_first / (jnp.sqrt(new_second) + EPSILON_ADAM)
    return (new_first, new_second, direction)


def column(row):
    return jnp.transpose(jnp.broadcast_to(row, (row.shape[1], row.shape[1])))


def bytes_of(ref, sem):
    pltpu.make_async_copy(ref, ref, sem).wait()


class Gather:
    def __init__(self, buf, send, recv, z, x):
        self.buf, self.send, self.recv = buf, send, recv
        self.pos = {"fs_0": z, "fs_1": x}
        self.rows = buf.shape[3]

    def at(self, half, where, part):
        rows = slice(None) if part is None else pl.ds(part * (self.rows // 2), self.rows // 2)
        first = where.get("fs_0", slice(None))
        second = where.get("fs_1", slice(None))
        return self.buf.at[first, second, half, rows]

    def copies(self, stage):
        phase, forward = divmod(stage, 2)
        out = []
        for half in range(2):
            order = FS if half == 0 else FS[::-1]
            axis = order[phase]
            other = order[1 - phase]
            for way in range(2):
                step = 1 if way == 0 else FS_SIDE - 1
                here = self.pos[axis]
                target = lax.rem(here + step, FS_SIDE)
                held = here if not forward else lax.rem(here + FS_SIDE - step, FS_SIDE)
                where = {axis: held}
                if phase == 0:
                    where[other] = self.pos[other]
                view = self.at(half, where, way if forward else None)
                out.append(
                    pltpu.make_async_remote_copy(
                        src_ref=view,
                        dst_ref=view,
                        send_sem=self.send.at[stage],
                        recv_sem=self.recv.at[stage],
                        device_id={axis: target},
                        device_id_type=MESH,
                    )
                )
        return out

    def start(self, stage):
        for copy in self.copies(stage):
            copy.start()

    def moved(self, stage):
        if stage == 0:
            return self.buf.at[0, 0:2]
        if stage == 1:
            return self.buf.at[0, 0]
        return self.buf.at[0:2] if stage == 2 else self.buf.at[0]

    def arrive(self, stage):
        bytes_of(self.moved(stage), self.recv.at[stage])

    def finish(self):
        for stage in range(4):
            bytes_of(self.moved(stage), self.send.at[stage])


def spread(z, x):
    for step in range(1, FS_COUNT):
        far_z = lax.rem(z + step // FS_SIDE, FS_SIDE)
        far_x = lax.rem(x + step % FS_SIDE, FS_SIDE)
        yield step, far_z, far_x


def shares_out(parts, landing, send, recv, z, x):
    return [
        pltpu.make_async_remote_copy(
            src_ref=parts.at[far_z * FS_SIDE + far_x],
            dst_ref=landing.at[step],
            send_sem=send,
            recv_sem=recv,
            device_id={"fs_0": far_z, "fs_1": far_x},
            device_id_type=MESH,
        )
        for step, far_z, far_x in spread(z, x)
    ]


def rows_out(rows, send, recv, z, x):
    mine = rows.at[z * FS_SIDE + x]
    return [
        pltpu.make_async_remote_copy(
            src_ref=mine,
            dst_ref=mine,
            send_sem=send,
            recv_sem=recv,
            device_id={"fs_0": far_z, "fs_1": far_x},
            device_id_type=MESH,
        )
        for step, far_z, far_x in spread(z, x)
    ]


def sums_out(sums, send, recv, y, c):
    return [
        pltpu.make_async_remote_copy(
            src_ref=sums.at[0],
            dst_ref=sums.at[step],
            send_sem=send,
            recv_sem=recv,
            device_id={
                "tp_0": lax.rem(y + step // 2, 4),
                "tp_1": lax.rem(c + step % 2, 2),
            },
            device_id_type=MESH,
        )
        for step in range(1, 8)
    ]


def totals_out(totals, send, recv, z, x):
    return [
        pltpu.make_async_remote_copy(
            src_ref=totals.at[0],
            dst_ref=totals.at[step],
            send_sem=send,
            recv_sem=recv,
            device_id={"fs_0": far_z, "fs_1": far_x},
            device_id_type=MESH,
        )
        for step, far_z, far_x in spread(z, x)
    ]


def start(copies):
    for copy in copies:
        copy.start()


def body(
    lam_hbm,
    gain_hbm,
    out_weight_hbm,
    value_weight_hbm,
    out_first_hbm,
    out_second_hbm,
    value_first_hbm,
    value_second_hbm,
    query_hbm,
    key_hbm,
    value_hbm,
    out_cot_hbm,
    layer_hbm,
    value_cot_hbm,
    out_basis_hbm,
    value_basis_hbm,
    out_step_hbm,
    value_step_hbm,
    new_out_weight_hbm,
    new_value_weight_hbm,
    out_copy_hbm,
    value_copy_hbm,
    new_out_first_hbm,
    new_out_second_hbm,
    new_value_first_hbm,
    new_value_second_hbm,
    lam_ref,
    gain_ref,
    out_weight_ref,
    value_weight_ref,
    out_first_ref,
    out_second_ref,
    value_first_ref,
    value_second_ref,
    out_step_ref,
    value_step_ref,
    new_out_weight_ref,
    new_value_weight_ref,
    out_copy_ref,
    value_copy_ref,
    new_out_first_ref,
    new_out_second_ref,
    new_value_first_ref,
    new_value_second_ref,
    query_ref,
    key_ref,
    value_ref,
    value_cot_ref,
    out_basis_ref,
    value_basis_ref,
    layer_ref,
    out_cot_ref,
    turned_ref,
    score_ref,
    weight_ref,
    head_ref,
    high_ref,
    low_ref,
    out_all_ref,
    value_parts,
    value_landing,
    value_rows,
    value_sums,
    value_totals,
    out_parts,
    out_landing,
    out_rows,
    out_sums,
    out_totals,
    out_full_ref,
    proj_ref,
    local_sem,
    store_sem,
    gather_out_send,
    gather_out_recv,
    gather_value_send,
    gather_value_recv,
    share_send,
    share_recv,
    row_send,
    row_recv,
    sum_send,
    sum_recv,
    total_send,
    total_recv,
):
    z, x = lax.axis_index("fs_0"), lax.axis_index("fs_1")
    y, c = lax.axis_index("tp_0"), lax.axis_index("tp_1")
    me = z * FS_SIDE + x
    chunks = SEQ // BLOCK

    def span(n):
        return slice(n * BLOCK, (n + 1) * BLOCK)

    local = []

    def fetch(src, dst):
        copy = pltpu.make_async_copy(src, dst, local_sem.at[len(local)])
        local.append(copy)
        copy.start()
        return copy

    def part(n):
        return slice(n * 2 * BLOCK, (n + 1) * 2 * BLOCK)

    stored = []

    def store(src, dst):
        copy = pltpu.make_async_copy(src, dst, store_sem.at[len(stored)])
        stored.append(copy)
        copy.start()

    got_weight = fetch(out_weight_hbm, out_weight_ref)
    got_value_basis = fetch(value_basis_hbm, value_basis_ref)
    got_layer = [fetch(layer_hbm.at[part(0)], layer_ref.at[part(0)])]
    got_value_cot = fetch(value_cot_hbm, value_cot_ref)
    for n in range(1, chunks // 2):
        got_layer.append(fetch(layer_hbm.at[part(n)], layer_ref.at[part(n)]))

    barrier = pltpu.get_barrier_semaphore()
    for _, far_z, far_x in spread(z, x):
        pl.semaphore_signal(
            barrier, inc=1, device_id={"fs_0": far_z, "fs_1": far_x}, device_id_type=MESH
        )
    for step in range(1, 8):
        pl.semaphore_signal(
            barrier,
            inc=1,
            device_id={"tp_0": lax.rem(y + step // 2, 4), "tp_1": lax.rem(c + step % 2, 2)},
            device_id_type=MESH,
        )
    got_weight.wait()
    out_all_ref[z, x, 0] = out_weight_ref[:128, :]
    out_all_ref[z, x, 1] = out_weight_ref[128:, :]

    gather_out = Gather(out_all_ref, gather_out_send, gather_out_recv, z, x)
    gather_value = Gather(value_copy_ref, gather_value_send, gather_value_recv, z, x)
    gathers = (gather_out, gather_value)
    value_shares = shares_out(value_parts, value_landing, share_send.at[0], share_recv.at[0], z, x)
    out_shares = shares_out(out_parts, out_landing, share_send.at[1], share_recv.at[1], z, x)
    value_row_copies = rows_out(value_rows, row_send.at[0], row_recv.at[0], z, x)
    out_row_copies = rows_out(out_rows, row_send.at[1], row_recv.at[1], z, x)
    value_sum_copies = sums_out(value_sums, sum_send.at[0], sum_recv.at[0], y, c)
    out_sum_copies = sums_out(out_sums, sum_send.at[1], sum_recv.at[1], y, c)
    value_total_copies = totals_out(value_totals, total_send.at[0], total_recv.at[0], z, x)
    out_total_copies = totals_out(out_totals, total_send.at[1], total_recv.at[1], z, x)

    def gather_next(gather, stage):
        gather.arrive(stage)
        if stage < 3:
            gather.start(stage + 1)

    got_value_basis.wait()
    for n in range(chunks // 2):
        got_layer[n].wait()
        if n == 1:
            got_value_cot.wait()
            pl.semaphore_wait(barrier, 22)
            gather_out.start(0)
        if n == 2:
            got_early = [
                fetch(lam_hbm, lam_ref),
                fetch(gain_hbm, gain_ref),
                fetch(query_hbm, query_ref),
                fetch(key_hbm, key_ref),
                fetch(value_hbm, value_ref),
            ]
        if n == 3:
            got_late = [
                fetch(out_basis_hbm, out_basis_ref),
                fetch(value_weight_hbm, value_weight_ref),
                fetch(value_first_hbm, value_first_ref),
                fetch(value_second_hbm, value_second_ref),
                fetch(out_first_hbm, out_first_ref),
                fetch(out_second_hbm, out_second_ref),
            ]
            got_out_cot = [
                fetch(out_cot_hbm.at[span(t)], out_cot_ref.at[span(t)]) for t in range(chunks)
            ]
        wide = mul(layer_ref[part(n), :], value_basis_ref[...])
        high_ref[part(n), :], low_ref[part(n), :] = two_parts(wide)
        if n == 1:
            for t in range(chunks):
                head_ref[:, span(t)] = value_cot_ref[span(t), :].T
    gather_next(gather_out, 0)
    proj_t = mul(head_ref[...], high_ref[...]) + mul(head_ref[...], low_ref[...])
    value_parts[...] = proj_t.T.reshape(FS_COUNT, SHARE, COLS)
    start(value_shares)

    for copy in got_early:
        copy.wait()
    turned_ref[:, span(0)] = value_ref[span(0), :].T
    gain = column(gain_ref[...])
    gain = jnp.concatenate([gain, gain], axis=1)
    lane = lax.broadcasted_iota(jnp.int32, (BLOCK, 128), 1)
    causal = lax.broadcasted_iota(jnp.int32, (BLOCK, BLOCK), 0) <= lax.broadcasted_iota(
        jnp.int32, (BLOCK, BLOCK), 1
    )

    jobs = [(i, h) for i in range(chunks) for h in range(2)]

    def scores(n, peaks):
        i, h = jobs[n]
        both = []
        for m in range(2):
            scaled = query_ref[span(i), h * 128 : (h + 1) * 128].astype(F32) * SCORE_SCALE
            scaled = jnp.where((lane < DH) if m == 0 else (lane >= DH), scaled, 0.0)
            both.append(jnp.concatenate(two_parts(scaled), axis=1))
        best = [None, None]
        for j in range(i + 1):
            keys = key_ref[span(j), h * 128 : (h + 1) * 128]
            for m in range(2):
                s = mul(jnp.concatenate([keys, keys], axis=1), both[m], NT)
                if j == i:
                    s = jnp.where(causal, s, -jnp.inf)
                score_ref[n % 2, m, span(j), :] = s
                top = jnp.max(s.reshape(BLOCK // 8, 8, BLOCK), axis=0)
                best[m] = top if best[m] is None else jnp.maximum(best[m], top)
                yield
        peaks.extend(jnp.max(b, axis=0, keepdims=True) for b in best)

    def weigh(n, peaks):
        i, h = jobs[n]
        held = score_ref.at[n % 2]
        sums = [None, None]
        for j in range(i + 1):
            for m in range(2):
                e = jnp.exp2(held[m, span(j), :] - peaks[m])
                part = jnp.sum(e.reshape(BLOCK // 8, 8, BLOCK), axis=0)
                sums[m] = part if sums[m] is None else sums[m] + part
                held[m, span(j), :] = e
                yield
        sums = [jnp.sum(t, axis=0, keepdims=True) for t in sums]
        one, two = 1.0 / sums[0], lam_ref[0:1, h : h + 1] / sums[1]
        for j in range(i + 1):
            mixed = held[0, span(j), :] * one - held[1, span(j), :] * two
            weight_ref[n % 2, span(j), :] = mixed.astype(BF16)
            yield
        depth = (i + 1) * BLOCK
        raw = mul(turned_ref[h * DV : (h + 1) * DV, :depth], weight_ref[n % 2, :depth, :])
        mean = jnp.mean(raw * raw, axis=0, keepdims=True)
        normed = raw * lax.rsqrt(mean + EPSILON_NORM) * gain
        head_ref[h * DV : (h + 1) * DV, span(i)] = normed.astype(BF16)

    def together(first, first_count, second, second_count):
        due = 0.0
        for _ in range(first_count):
            next(first, None)
            due += second_count / first_count
            while due >= 1.0:
                next(second, None)
                due -= 1.0
        for chain in (first, second):
            for _ in chain:
                pass

    def clip_of(totals):
        total = jnp.sum(jnp.sum(totals[...], axis=0), keepdims=True)
        return jnp.minimum(1.0, CLIP_RMS * math.sqrt(ENTRY_COUNT) / jnp.sqrt(total))

    def moments(parts, landing, first, second, new_first, new_second, rows, sums):
        proj = parts[me]
        for step in range(1, FS_COUNT):
            proj = proj + landing[step]
        new_first[...], new_second[...], direction = moment_step(proj, first[...], second[...])
        rows[me] = direction
        square = direction * direction
        sums[0] = square[:8, :128] + square[8:, :128] + square[:8, 128:] + square[8:, 128:]

    def after(n):
        if n == 2:
            gather_next(gather_out, 1)
        if n == 7:
            bytes_of(value_landing.at[0:15], share_recv.at[0])
            moments(
                value_parts,
                value_landing,
                value_first_ref,
                value_second_ref,
                new_value_first_ref,
                new_value_second_ref,
                value_rows,
                value_sums,
            )
            start(value_sum_copies)
            start(value_row_copies)
            store(new_value_first_ref, new_value_first_hbm)
            store(new_value_second_ref, new_value_second_hbm)
        if n == 11:
            bytes_of(value_sums.at[0:7], sum_recv.at[0])
            value_totals[0] = jnp.sum(value_sums[...], axis=0)
            start(value_total_copies)
        if n == 12:
            gather_next(gather_out, 2)
        if n == 14:
            bytes_of(value_rows.at[0:15], row_recv.at[0])
            bytes_of(value_totals.at[0:15], total_recv.at[0])
            high, low = two_parts(value_rows[...].reshape(RANK, COLS))
            own = value_basis_ref[pl.ds(pl.multiple_of(me * OWN, OWN), OWN), :]
            step = clip_of(value_totals) * (mul(own, high) + mul(own, low))
            value_step_ref[...] = step
            new = value_weight_ref[...] - LEARN_RATE * step
            new_value_weight_ref[...] = new
            value_copy_ref[z, x] = new.astype(BF16).reshape(2, OWN // 2, COLS)
            gather_value.start(0)
            store(value_step_ref, value_step_hbm)
            store(new_value_weight_ref, new_value_weight_hbm)

    def widen(n):
        wide = mul(out_cot_ref[span(n), :], out_basis_ref[...])
        high_ref[span(n), :], low_ref[span(n), :] = two_parts(wide)

    def project(low, high):
        rows = slice(low * BLOCK, high * BLOCK)
        return mul(head_ref[:, rows], high_ref[rows, :]) + mul(head_ref[:, rows], low_ref[rows, :])

    wide_at = {3: 0, 5: 1, 7: 2, 8: 3, 9: 4, 10: 5, 11: 6, 12: 7}

    def extra(n):
        i, h = jobs[n]
        if n in wide_at:
            widen(wide_at[n])
        if n == 13:
            proj_ref[...] = project(0, 5)
        if n == 15:
            proj_ref[...] += project(5, 7)
        if h == 1 and i + 1 < chunks:
            turned_ref[:, span(i + 1)] = value_ref[span(i + 1), :].T

    peaks = [[] for _ in jobs]
    for _ in scores(0, peaks[0]):
        pass
    for n, (i, h) in enumerate(jobs):
        if n == 3:
            for copy in got_late:
                copy.wait()
        if n in wide_at:
            got_out_cot[wide_at[n]].wait()
        extra(n)
        ahead, ahead_count = iter(()), 0
        if n + 1 < len(jobs):
            ahead, ahead_count = scores(n + 1, peaks[n + 1]), 2 * (jobs[n + 1][0] + 1) + 1
        together(weigh(n, peaks[n]), 3 * (i + 1) + 1, ahead, ahead_count)
        after(n)

    proj_t = proj_ref[...] + project(7, 8)
    out_parts[...] = proj_t.T.reshape(FS_COUNT, SHARE, COLS)
    start(out_shares)
    gather_next(gather_value, 0)
    gather_next(gather_value, 1)
    bytes_of(out_landing.at[0:15], share_recv.at[1])
    moments(
        out_parts,
        out_landing,
        out_first_ref,
        out_second_ref,
        new_out_first_ref,
        new_out_second_ref,
        out_rows,
        out_sums,
    )
    start(out_sum_copies)
    start(out_row_copies)
    store(new_out_first_ref, new_out_first_hbm)
    store(new_out_second_ref, new_out_second_hbm)
    gather_next(gather_value, 2)
    bytes_of(out_sums.at[0:7], sum_recv.at[1])
    out_totals[0] = jnp.sum(out_sums[...], axis=0)
    start(out_total_copies)
    gather_next(gather_out, 3)
    bytes_of(out_rows.at[0:15], row_recv.at[1])
    both = jnp.concatenate(two_parts(out_rows[...].reshape(RANK, COLS).T), axis=0)
    for n in range(chunks):
        full = mul(both, out_basis_ref[span(n), :], NT)
        out_full_ref[:, span(n)] = full[:COLS] + full[COLS:]
    gather_next(gather_value, 3)
    store(value_copy_ref, value_copy_hbm)
    bytes_of(out_totals.at[0:15], total_recv.at[1])
    clip = clip_of(out_totals)
    own = pl.ds(pl.multiple_of(me * OWN, OWN), OWN)
    step = clip * out_full_ref[:, own]
    out_step_ref[...] = step
    new_out_weight_ref[...] = out_weight_ref[...] - LEARN_RATE * step
    store(out_step_ref, out_step_hbm)
    store(new_out_weight_ref, new_out_weight_hbm)
    for at in range(FS_COUNT):
        old = out_all_ref[at // FS_SIDE, at % FS_SIDE].reshape(COLS, OWN)
        cols = slice(at * OWN, (at + 1) * OWN)
        new = old - LEARN_RATE * (clip * out_full_ref[:, cols])
        out_copy_ref[:, cols] = new.astype(BF16)
        if at % 8 == 7:
            half = slice((at - 7) * OWN, (at + 1) * OWN)
            store(out_copy_ref.at[:, half], out_copy_hbm.at[:, half])

    for gather in gathers:
        gather.finish()
    for k in range(2):
        bytes_of(value_landing.at[0:15], share_send.at[k])
        bytes_of(value_rows.at[0:15], row_send.at[k])
        bytes_of(value_sums.at[0:7], sum_send.at[k])
        bytes_of(value_totals.at[0:15], total_send.at[k])
    for copy in stored:
        copy.wait()


def hand_over(*refs):
    count = len(refs) // 3
    given, taken, held = refs[:count], refs[count : 2 * count], refs[2 * count : 3 * count]
    sems = refs[3 * count]
    loads = [pltpu.make_async_copy(a, b, sems.at[0, n]) for n, (a, b) in enumerate(zip(given, held))]
    stores = [pltpu.make_async_copy(a, b, sems.at[1, n]) for n, (a, b) in enumerate(zip(held, taken))]
    start(loads)
    for load, store in zip(loads, stores):
        load.wait()
        store.start()
    for store in stores:
        store.wait()


def results(arrays):
    anywhere = pl.BlockSpec(memory_space=pl.ANY)
    return pl.pallas_call(
        hand_over,
        out_shape=tuple(jax.ShapeDtypeStruct(a.shape, a.dtype) for a in arrays),
        in_specs=[anywhere] * len(arrays),
        out_specs=(anywhere,) * len(arrays),
        scratch_shapes=[pltpu.VMEM(a.shape, a.dtype) for a in arrays]
        + [pltpu.SemaphoreType.DMA((2, len(arrays)))],
    )(*arrays)


def step(
    query_rows,
    key_rows,
    value_rows,
    mix_lambda,
    head_gain,
    out_cotangent,
    layer_input,
    value_cotangent,
    out_weight,
    value_weight,
    out_basis,
    value_basis,
    out_first,
    out_second,
    value_first,
    value_second,
):
    anywhere = pl.BlockSpec(memory_space=pl.ANY)
    dma = pltpu.SemaphoreType.DMA
    shape = jax.ShapeDtypeStruct
    made = (
        shape((COLS, OWN), F32),
        shape((OWN, COLS), F32),
        shape((COLS, OWN), F32),
        shape((OWN, COLS), F32),
        shape((COLS, WIDE), BF16),
        shape((FS_SIDE, FS_SIDE, 2, OWN // 2, COLS), BF16),
        shape((SHARE, COLS), F32),
        shape((SHARE, COLS), F32),
        shape((SHARE, COLS), F32),
        shape((SHARE, COLS), F32),
    )
    arrays = pl.pallas_call(
        body,
        out_shape=made,
        in_specs=[anywhere] * 16,
        out_specs=(anywhere,) * 10,
        scratch_shapes=[
            pltpu.VMEM((1, 2), F32),
            pltpu.VMEM((1, DV), F32),
            pltpu.VMEM((COLS, OWN), F32),
            pltpu.VMEM((OWN, COLS), F32),
            *[pltpu.VMEM((SHARE, COLS), F32)] * 4,
            *[pltpu.VMEM(r.shape, r.dtype) for r in made],
            pltpu.VMEM((SEQ, COLS), BF16),
            pltpu.VMEM((SEQ, COLS), BF16),
            pltpu.VMEM((SEQ, COLS), BF16),
            pltpu.VMEM((SEQ, COLS), BF16),
            pltpu.VMEM((WIDE, RANK), BF16),
            pltpu.VMEM((WIDE, RANK), BF16),
            pltpu.VMEM((SEQ, WIDE), BF16),
            pltpu.VMEM((SEQ, WIDE), BF16),
            pltpu.VMEM((COLS, SEQ), BF16),
            pltpu.VMEM((2, 2, SEQ, BLOCK), F32),
            pltpu.VMEM((2, SEQ, BLOCK), BF16),
            pltpu.VMEM((COLS, SEQ), BF16),
            pltpu.VMEM((SEQ, RANK), BF16),
            pltpu.VMEM((SEQ, RANK), BF16),
            pltpu.VMEM((FS_SIDE, FS_SIDE, 2, COLS // 2, OWN), F32),
            pltpu.VMEM((FS_COUNT, SHARE, COLS), F32),
            pltpu.VMEM((FS_COUNT, SHARE, COLS), F32),
            pltpu.VMEM((FS_COUNT, SHARE, COLS), F32),
            pltpu.VMEM((8, 8, 128), F32),
            pltpu.VMEM((FS_COUNT, 8, 128), F32),
            pltpu.VMEM((FS_COUNT, SHARE, COLS), F32),
            pltpu.VMEM((FS_COUNT, SHARE, COLS), F32),
            pltpu.VMEM((FS_COUNT, SHARE, COLS), F32),
            pltpu.VMEM((8, 8, 128), F32),
            pltpu.VMEM((FS_COUNT, 8, 128), F32),
            pltpu.VMEM((COLS, WIDE), F32),
            pltpu.VMEM((COLS, RANK), F32),
            dma((27,)),
            dma((12,)),
            *[dma((4,))] * 4,
            *[dma((2,))] * 8,
        ],
        compiler_params=pltpu.CompilerParams(
            collective_id=0,
            has_side_effects=True,
            vmem_limit_bytes=62 * 2**20,
        ),
    )(
        mix_lambda.reshape(1, 2),
        head_gain.reshape(1, DV),
        out_weight,
        value_weight,
        out_first,
        out_second,
        value_first,
        value_second,
        query_rows,
        key_rows,
        value_rows,
        out_cotangent,
        layer_input,
        value_cotangent,
        out_basis,
        value_basis,
    )
    copy = arrays[5].reshape(WIDE, COLS)
    return results((*arrays[:5], copy, *arrays[6:]))


def solution(mesh):
    torus = Mesh(mesh.devices.reshape(4, 4, 4, 2), FS + TP)
    sliced = P(FS, TP)
    return jax.shard_map(
        step,
        mesh=torus,
        in_specs=(
            sliced,
            sliced,
            sliced,
            P(TP),
            P(),
            P(FS, None),
            P(FS, None),
            sliced,
            P(TP, FS),
            sliced,
            P(),
            P(),
            sliced,
            sliced,
            sliced,
            sliced,
        ),
        out_specs=(
            P(TP, FS),
            sliced,
            P(TP, FS),
            sliced,
            P(TP, None),
            P(None, TP),
            sliced,
            sliced,
            sliced,
            sliced,
        ),
        check_vma=False,
    )
```

```python
import math

import jax
import jax.numpy as jnp
from jax import lax
from jax.experimental import pallas as pl
from jax.experimental.pallas import tpu as pltpu
from jax.sharding import Mesh
from jax.sharding import PartitionSpec as P

FS = ("fs_0", "fs_1")
TP = ("tp_0", "tp_1")

SEQ = 2048
WIDE = 2048
COLS = 256
RANK = 256
BLOCK = 256
FS_SIDE = 4
FS_COUNT = 16
SHARE = RANK // FS_COUNT
OWN = WIDE // FS_COUNT
DH = 64
DV = 128

EPSILON_NORM = 1e-05
EPSILON_ADAM = 1e-08
BETA_ONE = 0.9
BETA_TWO = 0.95
CLIP_RMS = 1.0
LEARN_RATE = 0.01
ENTRY_COUNT = RANK * WIDE
SCORE_SCALE = math.log2(math.e) * DH**-0.5

F32 = jnp.float32
BF16 = jnp.bfloat16
MESH = pl.DeviceIdType.MESH
NT = (((1,), (1,)), ((), ()))
NN = (((1,), (0,)), ((), ()))


def mul(a, b, dims=NN):
    return lax.dot_general(a, b, dims, preferred_element_type=F32)


def two_parts(value):
    high = value.astype(BF16)
    return high, (value - high.astype(F32)).astype(BF16)


def moment_step(proj, first, second):
    new_first = BETA_ONE * first + (1.0 - BETA_ONE) * proj
    new_second = BETA_TWO * second + (1.0 - BETA_TWO) * proj * proj
    direction = new_first / (jnp.sqrt(new_second) + EPSILON_ADAM)
    return (new_first, new_second, direction)


def column(row):
    return jnp.transpose(jnp.broadcast_to(row, (row.shape[1], row.shape[1])))


def bytes_of(ref, sem):
    pltpu.make_async_copy(ref, ref, sem).wait()


class Gather:
    def __init__(self, buf, send, recv, z, x, early):
        self.early = early
        self.buf, self.send, self.recv = buf, send, recv
        self.pos = {"fs_0": z, "fs_1": x}
        self.rows = buf.shape[3]

    def at(self, half, where, part):
        rows = slice(None) if part is None else pl.ds(part * (self.rows // 2), self.rows // 2)
        first = where.get("fs_0", slice(None))
        second = where.get("fs_1", slice(None))
        return self.buf.at[first, second, half, rows]

    def copies(self, stage, ahead=(None,)):
        phase, forward = divmod(stage, 2)
        out = []
        for step in ahead:
            for half in range(2):
                order = FS if half == 0 else FS[::-1]
                axis = order[phase]
                other = order[1 - phase]
                for way in range(2):
                    hop = 1 if way == 0 else FS_SIDE - 1
                    here = self.pos[axis]
                    target = lax.rem(here + hop, FS_SIDE)
                    where = {axis: lax.rem(here + FS_SIDE - hop, FS_SIDE) if forward else here}
                    if phase == 0:
                        where[other] = self.pos[other]
                    elif step is not None:
                        where[other] = lax.rem(self.pos[other] + step, FS_SIDE)
                    view = self.at(half, where, way if forward else None)
                    out.append(
                        pltpu.make_async_remote_copy(
                            src_ref=view,
                            dst_ref=view,
                            send_sem=self.send.at[stage],
                            recv_sem=self.recv.at[stage],
                            device_id={axis: target},
                            device_id_type=MESH,
                        )
                    )
        return out

    def start(self, stage):
        if stage == 0:
            start(self.copies(0) + self.copies(2, (0,)))
        elif stage == 1:
            start(self.copies(1) + (self.copies(2, (1, 3)) if self.early else []))
        elif stage == 2:
            start(self.copies(2, (2,) if self.early else (1, 3, 2)))
        else:
            start(self.copies(3))

    def moved(self, stage):
        if stage == 0:
            return self.buf.at[0, 0:2]
        if stage == 1:
            return self.buf.at[0, 0]
        return self.buf.at[0:2] if stage == 2 else self.buf.at[0]

    def arrive(self, stage):
        bytes_of(self.moved(stage), self.recv.at[stage])

    def finish(self):
        for stage in range(4):
            bytes_of(self.moved(stage), self.send.at[stage])


def spread(z, x):
    for step in range(1, FS_COUNT):
        far_z = lax.rem(z + step // FS_SIDE, FS_SIDE)
        far_x = lax.rem(x + step % FS_SIDE, FS_SIDE)
        yield step, far_z, far_x


def shares_out(parts, landing, send, recv, z, x):
    return [
        pltpu.make_async_remote_copy(
            src_ref=parts.at[far_z * FS_SIDE + far_x],
            dst_ref=landing.at[step],
            send_sem=send,
            recv_sem=recv,
            device_id={"fs_0": far_z, "fs_1": far_x},
            device_id_type=MESH,
        )
        for step, far_z, far_x in spread(z, x)
    ]


def rows_out(rows, send, recv, z, x):
    mine = rows.at[z * FS_SIDE + x]
    return [
        pltpu.make_async_remote_copy(
            src_ref=mine,
            dst_ref=mine,
            send_sem=send,
            recv_sem=recv,
            device_id={"fs_0": far_z, "fs_1": far_x},
            device_id_type=MESH,
        )
        for step, far_z, far_x in spread(z, x)
    ]


def sums_out(sums, send, recv, y, c):
    return [
        pltpu.make_async_remote_copy(
            src_ref=sums.at[0],
            dst_ref=sums.at[step],
            send_sem=send,
            recv_sem=recv,
            device_id={
                "tp_0": lax.rem(y + step // 2, 4),
                "tp_1": lax.rem(c + step % 2, 2),
            },
            device_id_type=MESH,
        )
        for step in range(1, 8)
    ]


def totals_out(totals, send, recv, z, x):
    return [
        pltpu.make_async_remote_copy(
            src_ref=totals.at[0],
            dst_ref=totals.at[step],
            send_sem=send,
            recv_sem=recv,
            device_id={"fs_0": far_z, "fs_1": far_x},
            device_id_type=MESH,
        )
        for step, far_z, far_x in spread(z, x)
    ]


def start(copies):
    for copy in copies:
        copy.start()


def body(
    lam_hbm,
    gain_hbm,
    out_weight_hbm,
    value_weight_hbm,
    out_first_hbm,
    out_second_hbm,
    value_first_hbm,
    value_second_hbm,
    query_hbm,
    key_hbm,
    value_hbm,
    out_cot_hbm,
    layer_hbm,
    value_cot_hbm,
    out_basis_hbm,
    value_basis_hbm,
    out_step_hbm,
    value_step_hbm,
    new_out_weight_hbm,
    new_value_weight_hbm,
    out_copy_hbm,
    value_copy_hbm,
    new_out_first_hbm,
    new_out_second_hbm,
    new_value_first_hbm,
    new_value_second_hbm,
    lam_ref,
    gain_ref,
    out_weight_ref,
    value_weight_ref,
    out_first_ref,
    out_second_ref,
    value_first_ref,
    value_second_ref,
    out_step_ref,
    value_step_ref,
    new_out_weight_ref,
    new_value_weight_ref,
    out_copy_ref,
    value_copy_ref,
    new_out_first_ref,
    new_out_second_ref,
    new_value_first_ref,
    new_value_second_ref,
    query_ref,
    key_ref,
    value_ref,
    value_cot_ref,
    out_basis_ref,
    value_basis_ref,
    layer_ref,
    out_cot_ref,
    turned_ref,
    score_ref,
    weight_ref,
    head_ref,
    high_ref,
    low_ref,
    out_all_ref,
    value_parts,
    value_landing,
    value_rows,
    value_sums,
    value_totals,
    out_parts,
    out_landing,
    out_rows,
    out_sums,
    out_totals,
    out_full_ref,
    proj_ref,
    local_sem,
    store_sem,
    gather_out_send,
    gather_out_recv,
    gather_value_send,
    gather_value_recv,
    share_send,
    share_recv,
    row_send,
    row_recv,
    sum_send,
    sum_recv,
    total_send,
    total_recv,
):
    z, x = lax.axis_index("fs_0"), lax.axis_index("fs_1")
    y, c = lax.axis_index("tp_0"), lax.axis_index("tp_1")
    me = z * FS_SIDE + x
    chunks = SEQ // BLOCK

    def span(n):
        return slice(n * BLOCK, (n + 1) * BLOCK)

    local = []

    def fetch(src, dst):
        copy = pltpu.make_async_copy(src, dst, local_sem.at[len(local)])
        local.append(copy)
        copy.start()
        return copy

    def part(n):
        return slice(n * 2 * BLOCK, (n + 1) * 2 * BLOCK)

    stored = []

    def store(src, dst):
        copy = pltpu.make_async_copy(src, dst, store_sem.at[len(stored)])
        stored.append(copy)
        copy.start()

    got_weight = fetch(out_weight_hbm, out_weight_ref)
    got_value_basis = fetch(value_basis_hbm, value_basis_ref)
    got_layer = [fetch(layer_hbm.at[part(0)], layer_ref.at[part(0)])]
    got_value_cot = fetch(value_cot_hbm, value_cot_ref)
    for n in range(1, chunks // 2):
        got_layer.append(fetch(layer_hbm.at[part(n)], layer_ref.at[part(n)]))

    barrier = pltpu.get_barrier_semaphore()
    for _, far_z, far_x in spread(z, x):
        pl.semaphore_signal(
            barrier, inc=1, device_id={"fs_0": far_z, "fs_1": far_x}, device_id_type=MESH
        )
    for step in range(1, 8):
        pl.semaphore_signal(
            barrier,
            inc=1,
            device_id={"tp_0": lax.rem(y + step // 2, 4), "tp_1": lax.rem(c + step % 2, 2)},
            device_id_type=MESH,
        )
    got_weight.wait()
    out_all_ref[z, x, 0] = out_weight_ref[:128, :]
    out_all_ref[z, x, 1] = out_weight_ref[128:, :]

    gather_out = Gather(out_all_ref, gather_out_send, gather_out_recv, z, x, False)
    gather_value = Gather(value_copy_ref, gather_value_send, gather_value_recv, z, x, True)
    gathers = (gather_out, gather_value)
    value_shares = shares_out(value_parts, value_landing, share_send.at[0], share_recv.at[0], z, x)
    out_shares = shares_out(out_parts, out_landing, share_send.at[1], share_recv.at[1], z, x)
    value_row_copies = rows_out(value_rows, row_send.at[0], row_recv.at[0], z, x)
    out_row_copies = rows_out(out_rows, row_send.at[1], row_recv.at[1], z, x)
    value_sum_copies = sums_out(value_sums, sum_send.at[0], sum_recv.at[0], y, c)
    out_sum_copies = sums_out(out_sums, sum_send.at[1], sum_recv.at[1], y, c)
    value_total_copies = totals_out(value_totals, total_send.at[0], total_recv.at[0], z, x)
    out_total_copies = totals_out(out_totals, total_send.at[1], total_recv.at[1], z, x)

    def gather_next(gather, stage):
        gather.arrive(stage)
        if stage < 3:
            gather.start(stage + 1)

    got_value_basis.wait()
    for n in range(chunks // 2):
        got_layer[n].wait()
        if n == 1:
            got_value_cot.wait()
            pl.semaphore_wait(barrier, 22)
            gather_out.start(0)
        if n == 2:
            got_early = [
                fetch(lam_hbm, lam_ref),
                fetch(gain_hbm, gain_ref),
                fetch(query_hbm, query_ref),
                fetch(key_hbm, key_ref),
                fetch(value_hbm, value_ref),
            ]
        if n == 3:
            got_late = [
                fetch(out_basis_hbm, out_basis_ref),
                fetch(value_weight_hbm, value_weight_ref),
                fetch(value_first_hbm, value_first_ref),
                fetch(value_second_hbm, value_second_ref),
                fetch(out_first_hbm, out_first_ref),
                fetch(out_second_hbm, out_second_ref),
            ]
            got_out_cot = [
                fetch(out_cot_hbm.at[span(t)], out_cot_ref.at[span(t)]) for t in range(chunks)
            ]
        wide = mul(layer_ref[part(n), :], value_basis_ref[...])
        high_ref[part(n), :], low_ref[part(n), :] = two_parts(wide)
        if n == 1:
            for t in range(chunks):
                head_ref[:, span(t)] = value_cot_ref[span(t), :].T
    gather_next(gather_out, 0)
    proj_t = mul(head_ref[...], high_ref[...]) + mul(head_ref[...], low_ref[...])
    value_parts[...] = proj_t.T.reshape(FS_COUNT, SHARE, COLS)
    start(value_shares)

    for copy in got_early:
        copy.wait()
    turned_ref[:, span(0)] = value_ref[span(0), :].T
    gain = column(gain_ref[...])
    gain = jnp.concatenate([gain, gain], axis=1)
    lane = lax.broadcasted_iota(jnp.int32, (BLOCK, 128), 1)
    causal = lax.broadcasted_iota(jnp.int32, (BLOCK, BLOCK), 0) <= lax.broadcasted_iota(
        jnp.int32, (BLOCK, BLOCK), 1
    )

    jobs = [(i, h) for i in range(chunks) for h in range(2)]

    def scores(n, peaks):
        i, h = jobs[n]
        both = []
        for m in range(2):
            scaled = query_ref[span(i), h * 128 : (h + 1) * 128].astype(F32) * SCORE_SCALE
            scaled = jnp.where((lane < DH) if m == 0 else (lane >= DH), scaled, 0.0)
            both.append(jnp.concatenate(two_parts(scaled), axis=1))
        best = [None, None]
        for j in range(i + 1):
            keys = key_ref[span(j), h * 128 : (h + 1) * 128]
            for m in range(2):
                s = mul(jnp.concatenate([keys, keys], axis=1), both[m], NT)
                if j == i:
                    s = jnp.where(causal, s, -jnp.inf)
                score_ref[n % 2, m, span(j), :] = s
                top = jnp.max(s.reshape(BLOCK // 8, 8, BLOCK), axis=0)
                best[m] = top if best[m] is None else jnp.maximum(best[m], top)
                yield
        peaks.extend(jnp.max(b, axis=0, keepdims=True) for b in best)

    def weigh(n, peaks):
        i, h = jobs[n]
        held = score_ref.at[n % 2]
        sums = [None, None]
        for j in range(i + 1):
            for m in range(2):
                e = jnp.exp2(held[m, span(j), :] - peaks[m])
                part = jnp.sum(e.reshape(BLOCK // 8, 8, BLOCK), axis=0)
                sums[m] = part if sums[m] is None else sums[m] + part
                held[m, span(j), :] = e
                yield
        sums = [jnp.sum(t, axis=0, keepdims=True) for t in sums]
        one, two = 1.0 / sums[0], lam_ref[0:1, h : h + 1] / sums[1]
        for j in range(i + 1):
            mixed = held[0, span(j), :] * one - held[1, span(j), :] * two
            weight_ref[n % 2, span(j), :] = mixed.astype(BF16)
            yield
        depth = (i + 1) * BLOCK
        raw = mul(turned_ref[h * DV : (h + 1) * DV, :depth], weight_ref[n % 2, :depth, :])
        mean = jnp.mean(raw * raw, axis=0, keepdims=True)
        normed = raw * lax.rsqrt(mean + EPSILON_NORM) * gain
        head_ref[h * DV : (h + 1) * DV, span(i)] = normed.astype(BF16)

    def together(first, first_count, second, second_count):
        due = 0.0
        for _ in range(first_count):
            next(first, None)
            due += second_count / first_count
            while due >= 1.0:
                next(second, None)
                due -= 1.0
        for chain in (first, second):
            for _ in chain:
                pass

    def clip_of(totals):
        total = jnp.sum(jnp.sum(totals[...], axis=0), keepdims=True)
        return jnp.minimum(1.0, CLIP_RMS * math.sqrt(ENTRY_COUNT) / jnp.sqrt(total))

    def moments(parts, landing, first, second, new_first, new_second, rows, sums):
        proj = parts[me]
        for step in range(1, FS_COUNT):
            proj = proj + landing[step]
        new_first[...], new_second[...], direction = moment_step(proj, first[...], second[...])
        rows[me] = direction
        square = direction * direction
        sums[0] = square[:8, :128] + square[8:, :128] + square[:8, 128:] + square[8:, 128:]

    def after(n):
        if n == 4:
            gather_next(gather_out, 1)
        if n == 7:
            bytes_of(value_landing.at[0:15], share_recv.at[0])
            moments(
                value_parts,
                value_landing,
                value_first_ref,
                value_second_ref,
                new_value_first_ref,
                new_value_second_ref,
                value_rows,
                value_sums,
            )
            start(value_sum_copies)
            start(value_row_copies)
            store(new_value_first_ref, new_value_first_hbm)
            store(new_value_second_ref, new_value_second_hbm)
        if n == 11:
            bytes_of(value_sums.at[0:7], sum_recv.at[0])
            value_totals[0] = jnp.sum(value_sums[...], axis=0)
            start(value_total_copies)
        if n == 12:
            gather_next(gather_out, 2)
        if n == 14:
            bytes_of(value_rows.at[0:15], row_recv.at[0])
            bytes_of(value_totals.at[0:15], total_recv.at[0])
            high, low = two_parts(value_rows[...].reshape(RANK, COLS))
            own = value_basis_ref[pl.ds(pl.multiple_of(me * OWN, OWN), OWN), :]
            step = clip_of(value_totals) * (mul(own, high) + mul(own, low))
            value_step_ref[...] = step
            new = value_weight_ref[...] - LEARN_RATE * step
            new_value_weight_ref[...] = new
            value_copy_ref[z, x] = new.astype(BF16).reshape(2, OWN // 2, COLS)
            gather_value.start(0)
            store(value_step_ref, value_step_hbm)
            store(new_value_weight_ref, new_value_weight_hbm)

    def widen(n):
        wide = mul(out_cot_ref[span(n), :], out_basis_ref[...])
        high_ref[span(n), :], low_ref[span(n), :] = two_parts(wide)

    def project(low, high):
        rows = slice(low * BLOCK, high * BLOCK)
        return mul(head_ref[:, rows], high_ref[rows, :]) + mul(head_ref[:, rows], low_ref[rows, :])

    wide_at = {3: 0, 5: 1, 7: 2, 8: 3, 9: 4, 10: 5, 11: 6, 12: 7}

    def extra(n):
        i, h = jobs[n]
        if n in wide_at:
            widen(wide_at[n])
        if n == 13:
            proj_ref[...] = project(0, 5)
        if n == 15:
            proj_ref[...] += project(5, 7)
        if h == 1 and i + 1 < chunks:
            turned_ref[:, span(i + 1)] = value_ref[span(i + 1), :].T

    peaks = [[] for _ in jobs]
    for _ in scores(0, peaks[0]):
        pass
    for n, (i, h) in enumerate(jobs):
        if n == 3:
            for copy in got_late:
                copy.wait()
        if n in wide_at:
            got_out_cot[wide_at[n]].wait()
        extra(n)
        ahead, ahead_count = iter(()), 0
        if n + 1 < len(jobs):
            ahead, ahead_count = scores(n + 1, peaks[n + 1]), 2 * (jobs[n + 1][0] + 1) + 1
        together(weigh(n, peaks[n]), 3 * (i + 1) + 1, ahead, ahead_count)
        after(n)

    proj_t = proj_ref[...] + project(7, 8)
    out_parts[...] = proj_t.T.reshape(FS_COUNT, SHARE, COLS)
    start(out_shares)
    gather_next(gather_value, 0)
    gather_next(gather_value, 1)
    bytes_of(out_landing.at[0:15], share_recv.at[1])
    moments(
        out_parts,
        out_landing,
        out_first_ref,
        out_second_ref,
        new_out_first_ref,
        new_out_second_ref,
        out_rows,
        out_sums,
    )
    start(out_sum_copies)
    start(out_row_copies)
    store(new_out_first_ref, new_out_first_hbm)
    store(new_out_second_ref, new_out_second_hbm)
    bytes_of(out_sums.at[0:7], sum_recv.at[1])
    out_totals[0] = jnp.sum(out_sums[...], axis=0)
    start(out_total_copies)
    gather_next(gather_value, 2)
    gather_next(gather_out, 3)
    bytes_of(out_rows.at[0:15], row_recv.at[1])
    both = jnp.concatenate(two_parts(out_rows[...].reshape(RANK, COLS).T), axis=0)
    for n in range(chunks):
        full = mul(both, out_basis_ref[span(n), :], NT)
        out_full_ref[:, span(n)] = full[:COLS] + full[COLS:]
    bytes_of(out_totals.at[0:15], total_recv.at[1])
    clip = clip_of(out_totals)
    own = pl.ds(pl.multiple_of(me * OWN, OWN), OWN)
    step = clip * out_full_ref[:, own]
    out_step_ref[...] = step
    new_out_weight_ref[...] = out_weight_ref[...] - LEARN_RATE * step
    store(out_step_ref, out_step_hbm)
    store(new_out_weight_ref, new_out_weight_hbm)
    for at in range(FS_COUNT):
        old = out_all_ref[at // FS_SIDE, at % FS_SIDE].reshape(COLS, OWN)
        cols = slice(at * OWN, (at + 1) * OWN)
        new = old - LEARN_RATE * (clip * out_full_ref[:, cols])
        out_copy_ref[:, cols] = new.astype(BF16)
        if at % 8 == 7:
            half = slice((at - 7) * OWN, (at + 1) * OWN)
            store(out_copy_ref.at[:, half], out_copy_hbm.at[:, half])
    gather_next(gather_value, 3)
    store(value_copy_ref, value_copy_hbm)

    for gather in gathers:
        gather.finish()
    for k in range(2):
        bytes_of(value_landing.at[0:15], share_send.at[k])
        bytes_of(value_rows.at[0:15], row_send.at[k])
        bytes_of(value_sums.at[0:7], sum_send.at[k])
        bytes_of(value_totals.at[0:15], total_send.at[k])
    for copy in stored:
        copy.wait()


def hand_over(*refs):
    count = len(refs) // 3
    given, taken, held = refs[:count], refs[count : 2 * count], refs[2 * count : 3 * count]
    sems = refs[3 * count]
    loads = [pltpu.make_async_copy(a, b, sems.at[0, n]) for n, (a, b) in enumerate(zip(given, held))]
    stores = [pltpu.make_async_copy(a, b, sems.at[1, n]) for n, (a, b) in enumerate(zip(held, taken))]
    start(loads)
    for load, store in zip(loads, stores):
        load.wait()
        store.start()
    for store in stores:
        store.wait()


def results(arrays):
    anywhere = pl.BlockSpec(memory_space=pl.ANY)
    return pl.pallas_call(
        hand_over,
        out_shape=tuple(jax.ShapeDtypeStruct(a.shape, a.dtype) for a in arrays),
        in_specs=[anywhere] * len(arrays),
        out_specs=(anywhere,) * len(arrays),
        scratch_shapes=[pltpu.VMEM(a.shape, a.dtype) for a in arrays]
        + [pltpu.SemaphoreType.DMA((2, len(arrays)))],
    )(*arrays)


def step(
    query_rows,
    key_rows,
    value_rows,
    mix_lambda,
    head_gain,
    out_cotangent,
    layer_input,
    value_cotangent,
    out_weight,
    value_weight,
    out_basis,
    value_basis,
    out_first,
    out_second,
    value_first,
    value_second,
):
    anywhere = pl.BlockSpec(memory_space=pl.ANY)
    dma = pltpu.SemaphoreType.DMA
    shape = jax.ShapeDtypeStruct
    made = (
        shape((COLS, OWN), F32),
        shape((OWN, COLS), F32),
        shape((COLS, OWN), F32),
        shape((OWN, COLS), F32),
        shape((COLS, WIDE), BF16),
        shape((FS_SIDE, FS_SIDE, 2, OWN // 2, COLS), BF16),
        shape((SHARE, COLS), F32),
        shape((SHARE, COLS), F32),
        shape((SHARE, COLS), F32),
        shape((SHARE, COLS), F32),
    )
    arrays = pl.pallas_call(
        body,
        out_shape=made,
        in_specs=[anywhere] * 16,
        out_specs=(anywhere,) * 10,
        scratch_shapes=[
            pltpu.VMEM((1, 2), F32),
            pltpu.VMEM((1, DV), F32),
            pltpu.VMEM((COLS, OWN), F32),
            pltpu.VMEM((OWN, COLS), F32),
            *[pltpu.VMEM((SHARE, COLS), F32)] * 4,
            *[pltpu.VMEM(r.shape, r.dtype) for r in made],
            pltpu.VMEM((SEQ, COLS), BF16),
            pltpu.VMEM((SEQ, COLS), BF16),
            pltpu.VMEM((SEQ, COLS), BF16),
            pltpu.VMEM((SEQ, COLS), BF16),
            pltpu.VMEM((WIDE, RANK), BF16),
            pltpu.VMEM((WIDE, RANK), BF16),
            pltpu.VMEM((SEQ, WIDE), BF16),
            pltpu.VMEM((SEQ, WIDE), BF16),
            pltpu.VMEM((COLS, SEQ), BF16),
            pltpu.VMEM((2, 2, SEQ, BLOCK), F32),
            pltpu.VMEM((2, SEQ, BLOCK), BF16),
            pltpu.VMEM((COLS, SEQ), BF16),
            pltpu.VMEM((SEQ, RANK), BF16),
            pltpu.VMEM((SEQ, RANK), BF16),
            pltpu.VMEM((FS_SIDE, FS_SIDE, 2, COLS // 2, OWN), F32),
            pltpu.VMEM((FS_COUNT, SHARE, COLS), F32),
            pltpu.VMEM((FS_COUNT, SHARE, COLS), F32),
            pltpu.VMEM((FS_COUNT, SHARE, COLS), F32),
            pltpu.VMEM((8, 8, 128), F32),
            pltpu.VMEM((FS_COUNT, 8, 128), F32),
            pltpu.VMEM((FS_COUNT, SHARE, COLS), F32),
            pltpu.VMEM((FS_COUNT, SHARE, COLS), F32),
            pltpu.VMEM((FS_COUNT, SHARE, COLS), F32),
            pltpu.VMEM((8, 8, 128), F32),
            pltpu.VMEM((FS_COUNT, 8, 128), F32),
            pltpu.VMEM((COLS, WIDE), F32),
            pltpu.VMEM((COLS, RANK), F32),
            dma((27,)),
            dma((12,)),
            *[dma((4,))] * 4,
            *[dma((2,))] * 8,
        ],
        compiler_params=pltpu.CompilerParams(
            collective_id=0,
            has_side_effects=True,
            vmem_limit_bytes=62 * 2**20,
        ),
    )(
        mix_lambda.reshape(1, 2),
        head_gain.reshape(1, DV),
        out_weight,
        value_weight,
        out_first,
        out_second,
        value_first,
        value_second,
        query_rows,
        key_rows,
        value_rows,
        out_cotangent,
        layer_input,
        value_cotangent,
        out_basis,
        value_basis,
    )
    copy = arrays[5].reshape(WIDE, COLS)
    return results((*arrays[:5], copy, *arrays[6:]))


def solution(mesh):
    torus = Mesh(mesh.devices.reshape(4, 4, 4, 2), FS + TP)
    sliced = P(FS, TP)
    return jax.shard_map(
        step,
        mesh=torus,
        in_specs=(
            sliced,
            sliced,
            sliced,
            P(TP),
            P(),
            P(FS, None),
            P(FS, None),
            sliced,
            P(TP, FS),
            sliced,
            P(),
            P(),
            sliced,
            sliced,
            sliced,
            sliced,
        ),
        out_specs=(
            P(TP, FS),
            sliced,
            P(TP, FS),
            sliced,
            P(TP, None),
            P(None, TP),
            sliced,
            sliced,
            sliced,
            sliced,
        ),
        check_vma=False,
    )
```

```python
import math

import jax
import jax.numpy as jnp
from jax import lax
from jax.experimental import pallas as pl
from jax.experimental.pallas import tpu as pltpu
from jax.sharding import Mesh
from jax.sharding import PartitionSpec as P

FS = ("fs_0", "fs_1")
TP = ("tp_0", "tp_1")

SEQ = 2048
WIDE = 2048
COLS = 256
RANK = 256
BLOCK = 256
FS_SIDE = 4
FS_COUNT = 16
SHARE = RANK // FS_COUNT
OWN = WIDE // FS_COUNT
DH = 64
DV = 128

EPSILON_NORM = 1e-05
EPSILON_ADAM = 1e-08
BETA_ONE = 0.9
BETA_TWO = 0.95
CLIP_RMS = 1.0
LEARN_RATE = 0.01
ENTRY_COUNT = RANK * WIDE
SCORE_SCALE = math.log2(math.e) * DH**-0.5

F32 = jnp.float32
BF16 = jnp.bfloat16
MESH = pl.DeviceIdType.MESH
NT = (((1,), (1,)), ((), ()))
NN = (((1,), (0,)), ((), ()))


def mul(a, b, dims=NN):
    return lax.dot_general(a, b, dims, preferred_element_type=F32)


def two_parts(value):
    high = value.astype(BF16)
    return high, (value - high.astype(F32)).astype(BF16)


def moment_step(proj, first, second):
    new_first = BETA_ONE * first + (1.0 - BETA_ONE) * proj
    new_second = BETA_TWO * second + (1.0 - BETA_TWO) * proj * proj
    direction = new_first / (jnp.sqrt(new_second) + EPSILON_ADAM)
    return (new_first, new_second, direction)


def column(row):
    return jnp.transpose(jnp.broadcast_to(row, (row.shape[1], row.shape[1])))


def bytes_of(ref, sem):
    pltpu.make_async_copy(ref, ref, sem).wait()


class Gather:
    def __init__(self, buf, send, recv, z, x, early):
        self.early = early
        self.buf, self.send, self.recv = buf, send, recv
        self.pos = {"fs_0": z, "fs_1": x}
        self.rows = buf.shape[3]

    def at(self, half, where, part):
        rows = slice(None) if part is None else pl.ds(part * (self.rows // 2), self.rows // 2)
        first = where.get("fs_0", slice(None))
        second = where.get("fs_1", slice(None))
        return self.buf.at[first, second, half, rows]

    def copies(self, stage, ahead=(None,)):
        phase, forward = divmod(stage, 2)
        out = []
        for step in ahead:
            for half in range(2):
                order = FS if half == 0 else FS[::-1]
                axis = order[phase]
                other = order[1 - phase]
                for way in range(2):
                    hop = 1 if way == 0 else FS_SIDE - 1
                    here = self.pos[axis]
                    target = lax.rem(here + hop, FS_SIDE)
                    where = {axis: lax.rem(here + FS_SIDE - hop, FS_SIDE) if forward else here}
                    if phase == 0:
                        where[other] = self.pos[other]
                    elif step is not None:
                        where[other] = lax.rem(self.pos[other] + step, FS_SIDE)
                    view = self.at(half, where, way if forward else None)
                    out.append(
                        pltpu.make_async_remote_copy(
                            src_ref=view,
                            dst_ref=view,
                            send_sem=self.send.at[stage],
                            recv_sem=self.recv.at[stage],
                            device_id={axis: target},
                            device_id_type=MESH,
                        )
                    )
        return out

    def start(self, stage):
        if stage == 0:
            start(self.copies(0) + self.copies(2, (0,)))
        elif stage == 1:
            start(self.copies(1) + (self.copies(2, (1, 3)) if self.early else []))
        elif stage == 2:
            start(self.copies(2, (2,) if self.early else (1, 3, 2)))
        else:
            start(self.copies(3))

    def moved(self, stage):
        if stage == 0:
            return self.buf.at[0, 0:2]
        if stage == 1:
            return self.buf.at[0, 0]
        return self.buf.at[0:2] if stage == 2 else self.buf.at[0]

    def arrive(self, stage):
        bytes_of(self.moved(stage), self.recv.at[stage])

    def finish(self):
        for stage in range(4):
            bytes_of(self.moved(stage), self.send.at[stage])


def spread(z, x):
    for step in range(1, FS_COUNT):
        far_z = lax.rem(z + step // FS_SIDE, FS_SIDE)
        far_x = lax.rem(x + step % FS_SIDE, FS_SIDE)
        yield step, far_z, far_x


def shares_out(parts, landing, send, recv, z, x):
    return [
        pltpu.make_async_remote_copy(
            src_ref=parts.at[far_z * FS_SIDE + far_x],
            dst_ref=landing.at[step],
            send_sem=send,
            recv_sem=recv,
            device_id={"fs_0": far_z, "fs_1": far_x},
            device_id_type=MESH,
        )
        for step, far_z, far_x in spread(z, x)
    ]


def rows_out(rows, send, recv, z, x):
    mine = rows.at[z * FS_SIDE + x]
    return [
        pltpu.make_async_remote_copy(
            src_ref=mine,
            dst_ref=mine,
            send_sem=send,
            recv_sem=recv,
            device_id={"fs_0": far_z, "fs_1": far_x},
            device_id_type=MESH,
        )
        for step, far_z, far_x in spread(z, x)
    ]


def sums_out(sums, send, recv, y, c):
    return [
        pltpu.make_async_remote_copy(
            src_ref=sums.at[0],
            dst_ref=sums.at[step],
            send_sem=send,
            recv_sem=recv,
            device_id={
                "tp_0": lax.rem(y + step // 2, 4),
                "tp_1": lax.rem(c + step % 2, 2),
            },
            device_id_type=MESH,
        )
        for step in range(1, 8)
    ]


def totals_out(totals, send, recv, z, x):
    return [
        pltpu.make_async_remote_copy(
            src_ref=totals.at[0],
            dst_ref=totals.at[step],
            send_sem=send,
            recv_sem=recv,
            device_id={"fs_0": far_z, "fs_1": far_x},
            device_id_type=MESH,
        )
        for step, far_z, far_x in spread(z, x)
    ]


def start(copies):
    for copy in copies:
        copy.start()


def body(
    lam_hbm,
    gain_hbm,
    out_weight_hbm,
    value_weight_hbm,
    out_first_hbm,
    out_second_hbm,
    value_first_hbm,
    value_second_hbm,
    query_hbm,
    key_hbm,
    value_hbm,
    out_cot_hbm,
    layer_hbm,
    value_cot_hbm,
    out_basis_hbm,
    value_basis_hbm,
    out_step_hbm,
    value_step_hbm,
    new_out_weight_hbm,
    new_value_weight_hbm,
    out_copy_hbm,
    value_copy_hbm,
    new_out_first_hbm,
    new_out_second_hbm,
    new_value_first_hbm,
    new_value_second_hbm,
    lam_ref,
    gain_ref,
    out_weight_ref,
    value_weight_ref,
    out_first_ref,
    out_second_ref,
    value_first_ref,
    value_second_ref,
    out_step_ref,
    value_step_ref,
    new_out_weight_ref,
    new_value_weight_ref,
    out_copy_ref,
    value_copy_ref,
    new_out_first_ref,
    new_out_second_ref,
    new_value_first_ref,
    new_value_second_ref,
    query_ref,
    key_ref,
    value_ref,
    value_cot_ref,
    out_basis_ref,
    value_basis_ref,
    layer_ref,
    out_cot_ref,
    turned_ref,
    score_ref,
    weight_ref,
    head_ref,
    high_ref,
    low_ref,
    out_all_ref,
    value_parts,
    value_landing,
    value_rows,
    value_sums,
    value_totals,
    out_parts,
    out_landing,
    out_rows,
    out_sums,
    out_totals,
    out_full_ref,
    proj_ref,
    local_sem,
    store_sem,
    gather_out_send,
    gather_out_recv,
    gather_value_send,
    gather_value_recv,
    share_send,
    share_recv,
    row_send,
    row_recv,
    sum_send,
    sum_recv,
    total_send,
    total_recv,
):
    z, x = lax.axis_index("fs_0"), lax.axis_index("fs_1")
    y, c = lax.axis_index("tp_0"), lax.axis_index("tp_1")
    me = z * FS_SIDE + x
    chunks = SEQ // BLOCK

    def span(n):
        return slice(n * BLOCK, (n + 1) * BLOCK)

    local = []

    def fetch(src, dst):
        copy = pltpu.make_async_copy(src, dst, local_sem.at[len(local)])
        local.append(copy)
        copy.start()
        return copy

    parts = (0, 256, 768, 1280, 2048)

    def part(n):
        return slice(parts[n], parts[n + 1])

    stored = []

    def store(src, dst):
        copy = pltpu.make_async_copy(src, dst, store_sem.at[len(stored)])
        stored.append(copy)
        copy.start()

    got_weight = fetch(out_weight_hbm, out_weight_ref)
    got_value_basis = fetch(value_basis_hbm, value_basis_ref)
    got_layer = [fetch(layer_hbm.at[part(0)], layer_ref.at[part(0)])]
    for n in range(1, 4):
        got_layer.append(fetch(layer_hbm.at[part(n)], layer_ref.at[part(n)]))
    got_value_cot = fetch(value_cot_hbm, value_cot_ref)

    barrier = pltpu.get_barrier_semaphore()
    for _, far_z, far_x in spread(z, x):
        pl.semaphore_signal(
            barrier, inc=1, device_id={"fs_0": far_z, "fs_1": far_x}, device_id_type=MESH
        )
    for step in range(1, 8):
        pl.semaphore_signal(
            barrier,
            inc=1,
            device_id={"tp_0": lax.rem(y + step // 2, 4), "tp_1": lax.rem(c + step % 2, 2)},
            device_id_type=MESH,
        )
    got_weight.wait()
    out_all_ref[z, x, 0] = out_weight_ref[:128, :]
    out_all_ref[z, x, 1] = out_weight_ref[128:, :]

    gather_out = Gather(out_all_ref, gather_out_send, gather_out_recv, z, x, False)
    gather_value = Gather(value_copy_ref, gather_value_send, gather_value_recv, z, x, True)
    gathers = (gather_out, gather_value)
    value_shares = shares_out(value_parts, value_landing, share_send.at[0], share_recv.at[0], z, x)
    out_shares = shares_out(out_parts, out_landing, share_send.at[1], share_recv.at[1], z, x)
    value_row_copies = rows_out(value_rows, row_send.at[0], row_recv.at[0], z, x)
    out_row_copies = rows_out(out_rows, row_send.at[1], row_recv.at[1], z, x)
    value_sum_copies = sums_out(value_sums, sum_send.at[0], sum_recv.at[0], y, c)
    out_sum_copies = sums_out(out_sums, sum_send.at[1], sum_recv.at[1], y, c)
    value_total_copies = totals_out(value_totals, total_send.at[0], total_recv.at[0], z, x)
    out_total_copies = totals_out(out_totals, total_send.at[1], total_recv.at[1], z, x)

    def gather_next(gather, stage):
        gather.arrive(stage)
        if stage < 3:
            gather.start(stage + 1)

    got_value_basis.wait()
    for n in range(4):
        got_layer[n].wait()
        if n == 1:
            pl.semaphore_wait(barrier, 22)
            gather_out.start(0)
        if n == 2:
            got_early = [
                fetch(lam_hbm, lam_ref),
                fetch(gain_hbm, gain_ref),
                fetch(query_hbm, query_ref),
                fetch(key_hbm, key_ref),
                fetch(value_hbm, value_ref),
            ]
        if n == 3:
            got_value_cot.wait()
            got_late = [
                fetch(out_basis_hbm, out_basis_ref),
                fetch(value_weight_hbm, value_weight_ref),
                fetch(value_first_hbm, value_first_ref),
                fetch(value_second_hbm, value_second_ref),
                fetch(out_first_hbm, out_first_ref),
                fetch(out_second_hbm, out_second_ref),
            ]
            got_out_cot = [
                fetch(out_cot_hbm.at[span(t)], out_cot_ref.at[span(t)]) for t in range(chunks)
            ]
        wide = mul(layer_ref[part(n), :], value_basis_ref[...])
        high_ref[part(n), :], low_ref[part(n), :] = two_parts(wide)
        if n == 3:
            for t in range(chunks):
                head_ref[:, span(t)] = value_cot_ref[span(t), :].T
    gather_next(gather_out, 0)
    proj_t = mul(head_ref[...], high_ref[...]) + mul(head_ref[...], low_ref[...])
    value_parts[...] = proj_t.T.reshape(FS_COUNT, SHARE, COLS)
    start(value_shares)

    for copy in got_early:
        copy.wait()
    turned_ref[:, span(0)] = value_ref[span(0), :].T
    gain = column(gain_ref[...])
    gain = jnp.concatenate([gain, gain], axis=1)
    lane = lax.broadcasted_iota(jnp.int32, (BLOCK, 128), 1)
    causal = lax.broadcasted_iota(jnp.int32, (BLOCK, BLOCK), 0) <= lax.broadcasted_iota(
        jnp.int32, (BLOCK, BLOCK), 1
    )

    jobs = [(i, h) for i in range(chunks) for h in range(2)]

    def scores(n, peaks):
        i, h = jobs[n]
        both = []
        for m in range(2):
            scaled = query_ref[span(i), h * 128 : (h + 1) * 128].astype(F32) * SCORE_SCALE
            scaled = jnp.where((lane < DH) if m == 0 else (lane >= DH), scaled, 0.0)
            both.append(jnp.concatenate(two_parts(scaled), axis=1))
        best = [None, None]
        for j in range(i + 1):
            keys = key_ref[span(j), h * 128 : (h + 1) * 128]
            for m in range(2):
                s = mul(jnp.concatenate([keys, keys], axis=1), both[m], NT)
                if j == i:
                    s = jnp.where(causal, s, -jnp.inf)
                score_ref[n % 2, m, span(j), :] = s
                top = jnp.max(s.reshape(BLOCK // 8, 8, BLOCK), axis=0)
                best[m] = top if best[m] is None else jnp.maximum(best[m], top)
                yield
        peaks.extend(jnp.max(b, axis=0, keepdims=True) for b in best)

    def weigh(n, peaks):
        i, h = jobs[n]
        held = score_ref.at[n % 2]
        sums = [None, None]
        for j in range(i + 1):
            for m in range(2):
                e = jnp.exp2(held[m, span(j), :] - peaks[m])
                part = jnp.sum(e.reshape(BLOCK // 8, 8, BLOCK), axis=0)
                sums[m] = part if sums[m] is None else sums[m] + part
                held[m, span(j), :] = e
                yield
        sums = [jnp.sum(t, axis=0, keepdims=True) for t in sums]
        one, two = 1.0 / sums[0], lam_ref[0:1, h : h + 1] / sums[1]
        for j in range(i + 1):
            mixed = held[0, span(j), :] * one - held[1, span(j), :] * two
            weight_ref[n % 2, span(j), :] = mixed.astype(BF16)
            yield
        depth = (i + 1) * BLOCK
        raw = mul(turned_ref[h * DV : (h + 1) * DV, :depth], weight_ref[n % 2, :depth, :])
        mean = jnp.mean(raw * raw, axis=0, keepdims=True)
        normed = raw * lax.rsqrt(mean + EPSILON_NORM) * gain
        head_ref[h * DV : (h + 1) * DV, span(i)] = normed.astype(BF16)

    def together(first, first_count, second, second_count):
        due = 0.0
        for _ in range(first_count):
            next(first, None)
            due += second_count / first_count
            while due >= 1.0:
                next(second, None)
                due -= 1.0
        for chain in (first, second):
            for _ in chain:
                pass

    def clip_of(totals):
        total = jnp.sum(jnp.sum(totals[...], axis=0), keepdims=True)
        return jnp.minimum(1.0, CLIP_RMS * math.sqrt(ENTRY_COUNT) / jnp.sqrt(total))

    def moments(parts, landing, first, second, new_first, new_second, rows, sums):
        proj = parts[me]
        for step in range(1, FS_COUNT):
            proj = proj + landing[step]
        new_first[...], new_second[...], direction = moment_step(proj, first[...], second[...])
        rows[me] = direction
        square = direction * direction
        sums[0] = square[:8, :128] + square[8:, :128] + square[:8, 128:] + square[8:, 128:]

    def after(n):
        if n == 4:
            gather_next(gather_out, 1)
        if n == 7:
            bytes_of(value_landing.at[0:15], share_recv.at[0])
            moments(
                value_parts,
                value_landing,
                value_first_ref,
                value_second_ref,
                new_value_first_ref,
                new_value_second_ref,
                value_rows,
                value_sums,
            )
            start(value_sum_copies)
            start(value_row_copies)
            store(new_value_first_ref, new_value_first_hbm)
            store(new_value_second_ref, new_value_second_hbm)
        if n == 11:
            bytes_of(value_sums.at[0:7], sum_recv.at[0])
            value_totals[0] = jnp.sum(value_sums[...], axis=0)
            start(value_total_copies)
        if n == 12:
            gather_next(gather_out, 2)
        if n == 14:
            bytes_of(value_rows.at[0:15], row_recv.at[0])
            bytes_of(value_totals.at[0:15], total_recv.at[0])
            high, low = two_parts(value_rows[...].reshape(RANK, COLS))
            own = value_basis_ref[pl.ds(pl.multiple_of(me * OWN, OWN), OWN), :]
            step = clip_of(value_totals) * (mul(own, high) + mul(own, low))
            value_step_ref[...] = step
            new = value_weight_ref[...] - LEARN_RATE * step
            new_value_weight_ref[...] = new
            value_copy_ref[z, x] = new.astype(BF16).reshape(2, OWN // 2, COLS)
            gather_value.start(0)
            store(value_step_ref, value_step_hbm)
            store(new_value_weight_ref, new_value_weight_hbm)

    def widen(n):
        wide = mul(out_cot_ref[span(n), :], out_basis_ref[...])
        high_ref[span(n), :], low_ref[span(n), :] = two_parts(wide)

    def project(low, high):
        rows = slice(low * BLOCK, high * BLOCK)
        return mul(head_ref[:, rows], high_ref[rows, :]) + mul(head_ref[:, rows], low_ref[rows, :])

    wide_at = {3: 0, 5: 1, 7: 2, 8: 3, 9: 4, 10: 5, 11: 6, 12: 7}

    def extra(n):
        i, h = jobs[n]
        if n in wide_at:
            widen(wide_at[n])
        if n == 13:
            proj_ref[...] = project(0, 5)
        if n == 15:
            proj_ref[...] += project(5, 7)
        if h == 1 and i + 1 < chunks:
            turned_ref[:, span(i + 1)] = value_ref[span(i + 1), :].T

    peaks = [[] for _ in jobs]
    for _ in scores(0, peaks[0]):
        pass
    for n, (i, h) in enumerate(jobs):
        if n == 3:
            for copy in got_late:
                copy.wait()
        if n in wide_at:
            got_out_cot[wide_at[n]].wait()
        extra(n)
        ahead, ahead_count = iter(()), 0
        if n + 1 < len(jobs):
            ahead, ahead_count = scores(n + 1, peaks[n + 1]), 2 * (jobs[n + 1][0] + 1) + 1
        together(weigh(n, peaks[n]), 3 * (i + 1) + 1, ahead, ahead_count)
        after(n)

    proj_t = proj_ref[...] + project(7, 8)
    out_parts[...] = proj_t.T.reshape(FS_COUNT, SHARE, COLS)
    start(out_shares)
    gather_next(gather_value, 0)
    gather_next(gather_value, 1)
    bytes_of(out_landing.at[0:15], share_recv.at[1])
    moments(
        out_parts,
        out_landing,
        out_first_ref,
        out_second_ref,
        new_out_first_ref,
        new_out_second_ref,
        out_rows,
        out_sums,
    )
    start(out_sum_copies)
    start(out_row_copies)
    store(new_out_first_ref, new_out_first_hbm)
    store(new_out_second_ref, new_out_second_hbm)
    bytes_of(out_sums.at[0:7], sum_recv.at[1])
    out_totals[0] = jnp.sum(out_sums[...], axis=0)
    start(out_total_copies)
    gather_next(gather_value, 2)
    gather_next(gather_out, 3)
    bytes_of(out_rows.at[0:15], row_recv.at[1])
    both = jnp.concatenate(two_parts(out_rows[...].reshape(RANK, COLS).T), axis=0)
    for n in range(chunks):
        full = mul(both, out_basis_ref[span(n), :], NT)
        out_full_ref[:, span(n)] = full[:COLS] + full[COLS:]
    bytes_of(out_totals.at[0:15], total_recv.at[1])
    clip = clip_of(out_totals)
    own = pl.ds(pl.multiple_of(me * OWN, OWN), OWN)
    step = clip * out_full_ref[:, own]
    out_step_ref[...] = step
    new_out_weight_ref[...] = out_weight_ref[...] - LEARN_RATE * step
    store(out_step_ref, out_step_hbm)
    store(new_out_weight_ref, new_out_weight_hbm)
    for at in range(FS_COUNT):
        old = out_all_ref[at // FS_SIDE, at % FS_SIDE].reshape(COLS, OWN)
        cols = slice(at * OWN, (at + 1) * OWN)
        new = old - LEARN_RATE * (clip * out_full_ref[:, cols])
        out_copy_ref[:, cols] = new.astype(BF16)
        if at % 4 == 3:
            cols = slice((at - 3) * OWN, (at + 1) * OWN)
            store(out_copy_ref.at[:, cols], out_copy_hbm.at[:, cols])
    gather_next(gather_value, 3)
    store(value_copy_ref, value_copy_hbm)

    for gather in gathers:
        gather.finish()
    for k in range(2):
        bytes_of(value_landing.at[0:15], share_send.at[k])
        bytes_of(value_rows.at[0:15], row_send.at[k])
        bytes_of(value_sums.at[0:7], sum_send.at[k])
        bytes_of(value_totals.at[0:15], total_send.at[k])
    for copy in stored:
        copy.wait()


def hand_over(*refs):
    count = len(refs) // 3
    given, taken, held = refs[:count], refs[count : 2 * count], refs[2 * count : 3 * count]
    sems = refs[3 * count]
    loads = [pltpu.make_async_copy(a, b, sems.at[0, n]) for n, (a, b) in enumerate(zip(given, held))]
    stores = [pltpu.make_async_copy(a, b, sems.at[1, n]) for n, (a, b) in enumerate(zip(held, taken))]
    start(loads)
    for load, store in zip(loads, stores):
        load.wait()
        store.start()
    for store in stores:
        store.wait()


def results(arrays):
    anywhere = pl.BlockSpec(memory_space=pl.ANY)
    return pl.pallas_call(
        hand_over,
        out_shape=tuple(jax.ShapeDtypeStruct(a.shape, a.dtype) for a in arrays),
        in_specs=[anywhere] * len(arrays),
        out_specs=(anywhere,) * len(arrays),
        scratch_shapes=[pltpu.VMEM(a.shape, a.dtype) for a in arrays]
        + [pltpu.SemaphoreType.DMA((2, len(arrays)))],
    )(*arrays)


def step(
    query_rows,
    key_rows,
    value_rows,
    mix_lambda,
    head_gain,
    out_cotangent,
    layer_input,
    value_cotangent,
    out_weight,
    value_weight,
    out_basis,
    value_basis,
    out_first,
    out_second,
    value_first,
    value_second,
):
    anywhere = pl.BlockSpec(memory_space=pl.ANY)
    dma = pltpu.SemaphoreType.DMA
    shape = jax.ShapeDtypeStruct
    made = (
        shape((COLS, OWN), F32),
        shape((OWN, COLS), F32),
        shape((COLS, OWN), F32),
        shape((OWN, COLS), F32),
        shape((COLS, WIDE), BF16),
        shape((FS_SIDE, FS_SIDE, 2, OWN // 2, COLS), BF16),
        shape((SHARE, COLS), F32),
        shape((SHARE, COLS), F32),
        shape((SHARE, COLS), F32),
        shape((SHARE, COLS), F32),
    )
    arrays = pl.pallas_call(
        body,
        out_shape=made,
        in_specs=[anywhere] * 16,
        out_specs=(anywhere,) * 10,
        scratch_shapes=[
            pltpu.VMEM((1, 2), F32),
            pltpu.VMEM((1, DV), F32),
            pltpu.VMEM((COLS, OWN), F32),
            pltpu.VMEM((OWN, COLS), F32),
            *[pltpu.VMEM((SHARE, COLS), F32)] * 4,
            *[pltpu.VMEM(r.shape, r.dtype) for r in made],
            pltpu.VMEM((SEQ, COLS), BF16),
            pltpu.VMEM((SEQ, COLS), BF16),
            pltpu.VMEM((SEQ, COLS), BF16),
            pltpu.VMEM((SEQ, COLS), BF16),
            pltpu.VMEM((WIDE, RANK), BF16),
            pltpu.VMEM((WIDE, RANK), BF16),
            pltpu.VMEM((SEQ, WIDE), BF16),
            pltpu.VMEM((SEQ, WIDE), BF16),
            pltpu.VMEM((COLS, SEQ), BF16),
            pltpu.VMEM((2, 2, SEQ, BLOCK), F32),
            pltpu.VMEM((2, SEQ, BLOCK), BF16),
            pltpu.VMEM((COLS, SEQ), BF16),
            pltpu.VMEM((SEQ, RANK), BF16),
            pltpu.VMEM((SEQ, RANK), BF16),
            pltpu.VMEM((FS_SIDE, FS_SIDE, 2, COLS // 2, OWN), F32),
            pltpu.VMEM((FS_COUNT, SHARE, COLS), F32),
            pltpu.VMEM((FS_COUNT, SHARE, COLS), F32),
            pltpu.VMEM((FS_COUNT, SHARE, COLS), F32),
            pltpu.VMEM((8, 8, 128), F32),
            pltpu.VMEM((FS_COUNT, 8, 128), F32),
            pltpu.VMEM((FS_COUNT, SHARE, COLS), F32),
            pltpu.VMEM((FS_COUNT, SHARE, COLS), F32),
            pltpu.VMEM((FS_COUNT, SHARE, COLS), F32),
            pltpu.VMEM((8, 8, 128), F32),
            pltpu.VMEM((FS_COUNT, 8, 128), F32),
            pltpu.VMEM((COLS, WIDE), F32),
            pltpu.VMEM((COLS, RANK), F32),
            dma((27,)),
            dma((13,)),
            *[dma((4,))] * 4,
            *[dma((2,))] * 8,
        ],
        compiler_params=pltpu.CompilerParams(
            collective_id=0,
            has_side_effects=True,
            vmem_limit_bytes=62 * 2**20,
        ),
    )(
        mix_lambda.reshape(1, 2),
        head_gain.reshape(1, DV),
        out_weight,
        value_weight,
        out_first,
        out_second,
        value_first,
        value_second,
        query_rows,
        key_rows,
        value_rows,
        out_cotangent,
        layer_input,
        value_cotangent,
        out_basis,
        value_basis,
    )
    copy = arrays[5].reshape(WIDE, COLS)
    return results((*arrays[:5], copy, *arrays[6:]))


def solution(mesh):
    torus = Mesh(mesh.devices.reshape(4, 4, 4, 2), FS + TP)
    sliced = P(FS, TP)
    return jax.shard_map(
        step,
        mesh=torus,
        in_specs=(
            sliced,
            sliced,
            sliced,
            P(TP),
            P(),
            P(FS, None),
            P(FS, None),
            sliced,
            P(TP, FS),
            sliced,
            P(),
            P(),
            sliced,
            sliced,
            sliced,
            sliced,
        ),
        out_specs=(
            P(TP, FS),
            sliced,
            P(TP, FS),
            sliced,
            P(TP, None),
            P(None, TP),
            sliced,
            sliced,
            sliced,
            sliced,
        ),
        check_vma=False,
    )
```
